256 devices in a mesh: ep: 16 (over y, x), tp: 16 (over z, core).
Axes of the slice: x: 4, y: 4, z: 8, core: 2. Of those that a mesh axis runs over, the one named last changes fastest.
Arguments:
- queries: bfloat16 [16384, 1024], P('ep', 'tp'), may hold values from -8 to 8
- keys: bfloat16 [16384, 256], P('ep'), may hold values from -8 to 8
- values: bfloat16 [16384, 256], P('ep'), may hold values from -6 to 6
- query_gain: float32 [64], replicated, may hold values from 1 to 10
- key_gain: float32 [64], replicated, may hold values from 1 to 10
- moe_input: bfloat16 [12288, 2048], P(('ep', 'tp')), may hold values from -6 to 6
- expert_ids: int32 [12288, 2], P('ep'), may hold values from 0 to 15, all different within a row; in each aligned block of 48 rows (0 to 47, 48 to 95, ...) at most 7 rows name the same one
- route_weight: float32 [12288, 2], P('ep'), may hold values from 0.2 to 1
- gate_weight: bfloat16 [16, 2048, 7168], P('ep', None, 'tp'), may hold values from -0.125 to 0.125
- up_weight: bfloat16 [16, 2048, 7168], P('ep', None, 'tp'), may hold values from -0.125 to 0.125
- down_weight: bfloat16 [16, 7168, 2048], P('ep', 'tp'), may hold values from -0.0625 to 0.0625
- output_gain: float32 [2048], replicated, may hold values from 0.1 to 1.9
Outputs:
- attended: bfloat16 [16384, 1024], P('ep', 'tp')
- moe_output: bfloat16 [12288, 2048], P(('ep', 'tp'))
The draws below stay inside these ranges and needn't reach their ends.
Inputs may be any that keep to these rules, and one draw needn't show every extreme that they name: `expert_ids`: the 2 experts of a token differ. In the rows of one device (aligned blocks of 48 tokens) no expert is named by more than 7 tokens, and in every draw some expert is named by exactly 7 tokens of some device.
All inputs are finite; a program needn't handle non-finite values.
Results may differ from the reference program's by a relative error of at most 0.0085.
The reference program's roundings to bfloat16 on the way count: a program that leaves them out, or rounds other values in their place, can miss the bound.
Values may be sent and summed in bfloat16 or wider, within the bound.
A program may use at most 128 MiB of HBM per device.

```python
import math
import jax
import jax.numpy as jnp
import numpy as np
from jax import lax

D = 2048
HD = 64
QH = 16
KV = 4
GRID_W = 64
H_E = 7168
TOPK = 2
TOK_DEV = 48
LEN = 16384
TOKENS_B = 12288
EXPERTS = 16
CAP = 7
N_EP = 16
N_TP = 16


def draw_keys(key, part):
    normals = jax.random.normal(jax.random.fold_in(key, 31), (LEN, KV * HD), jnp.float32)
    return jnp.clip(normals, -8.0, 8.0).astype(jnp.bfloat16)


def draw_queries(key, part):
    normals = jax.random.normal(jax.random.fold_in(key, 33), (LEN, QH * HD), jnp.float32)
    return jnp.clip(normals, -8.0, 8.0).astype(jnp.bfloat16)


def draw_query_gain(key, part):
    seed_key = jax.random.fold_in(key, 41)
    return jnp.exp(jax.random.uniform(seed_key, (HD,), jnp.float32, 0.0, math.log(2.2)))


def draw_key_gain(key, part):
    seed_key = jax.random.fold_in(key, 43)
    return jnp.exp(jax.random.uniform(seed_key, (HD,), jnp.float32, 0.0, math.log(2.2)))


def block_levels(rng, shape, shards, low, largest):
    loudness = 1.0
    for dim, parts in shards:
        steps = jax.random.uniform(jax.random.fold_in(jax.random.fold_in(rng, 6), dim), (parts,), jnp.float32, low / len(shards), largest / len(shards))
        loudness = loudness * jnp.repeat(jnp.exp(steps), shape[dim] // parts).reshape((-1,) + (1,) * (len(shape) - 1 - dim))
    return loudness


def assign_block(key, own, number, rows, count, top, limit, slope):
    sequence = jax.random.permutation(key, count)
    heavy_load, usual = portions_of(count, rows * top, limit, slope, True), portions_of(count, rows * top, limit, slope, False)
    places = jnp.arange(count)

    def named(tallies, turn):
        used = int((tallies > 0).sum())
        fixed = max(1, used // 4)
        moved = fixed + (places - fixed + turn * (used - fixed)) % max(1, count - fixed)
        return jnp.zeros((count,), jnp.int32).at[sequence[jnp.where(places < fixed, places, moved)]].set(jnp.asarray(tallies, jnp.int32))

    tallies = jnp.where(number % 4 == 0, named(heavy_load, number // 4), named(usual, number - number // 4 - 1))
    mixed = jax.random.permutation(jax.random.fold_in(own, 3), count)
    source_of, sink = mixed[0:count // 2 * 2:2], mixed[1:count // 2 * 2:2]
    room = jnp.minimum(tallies[source_of] - 1, limit - tallies[sink]) // 2
    room = jnp.where((source_of == sequence[0]) | (sink == sequence[0]) | (tallies[sink] == 0), 0, jnp.maximum(room, 0))
    moved = jax.random.randint(jax.random.fold_in(own, 4), (count // 2,), 0, 1 << 20) % (room + 1)
    tallies = tallies.at[source_of].add(-moved).at[sink].add(moved)
    labels = jnp.searchsorted(jnp.cumsum(tallies), jnp.arange(rows * top), side="right").astype(jnp.int32)
    table = labels.reshape(top, rows).T
    table = table[jax.random.permutation(jax.random.fold_in(own, 1), rows)]
    turn = jax.random.randint(jax.random.fold_in(own, 2), (rows, 1), 0, top)
    return jnp.take_along_axis(table, (jnp.arange(top)[None, :] + turn) % top, axis=1)


def portions_of(number_of, total, limit, skew, full):
    portions = [(1 << 20) // math.isqrt(grade ** skew) + 1 for grade in range(1, number_of + 1)]
    largest = limit if full else min(limit, max(-(-total // number_of), total * portions[0] // sum(portions)))
    least = 1 if total - largest >= number_of - 1 else 0
    counts, spare = [largest] + [least] * (number_of - 1), total - largest - least * (number_of - 1)
    while spare > 0:
        movable = [i for i in range(1, number_of) if counts[i] < largest] or [i for i in range(1, number_of) if counts[i] < limit]
        mass, remaining = sum([portions[i] for i in movable]), spare
        for i in movable:
            addition = min(limit - counts[i], max(1, remaining * portions[i] // mass), spare)
            counts[i] = counts[i] + addition
            spare = spare - addition
    return np.array(counts)


def centred(own_key, dims, scale, reach, shards=(), held_as=jnp.bfloat16):
    level = block_levels(own_key, dims, shards, -0.22, 0.18) if shards else 1.0
    drawn = jax.random.normal(own_key, dims, jnp.float32) * scale * level
    return jnp.minimum(jnp.maximum(drawn, -reach), reach).astype(held_as)


def setup_inputs(seed: int = 0) -> dict:
    seeds = jax.random.split(jax.random.key(seed), 13)
    queries = draw_queries(jax.random.fold_in(seeds[12], 71), 0)
    keys = draw_keys(jax.random.fold_in(seeds[12], 71), 0)
    values = centred(seeds[2], (LEN, KV * HD), 1.0, 6.0, ((0, 16),))
    query_gain = draw_query_gain(jax.random.fold_in(seeds[12], 71), 0)
    key_gain = draw_key_gain(jax.random.fold_in(seeds[12], 71), 0)
    moe_input = centred(seeds[5], (TOKENS_B, D), 1.0, 6.0, ((0, 256),))
    expert_ids_keys = jax.random.split(jax.random.fold_in(seeds[6], 1), TOKENS_B // TOK_DEV)
    expert_ids_turns = jax.random.permutation(jax.random.fold_in(seeds[6], 3), TOKENS_B // TOK_DEV)
    expert_ids = jax.vmap(lambda own, number: assign_block(jax.random.fold_in(seeds[6], 2), own, number, TOK_DEV, EXPERTS, TOPK, CAP, 1))(expert_ids_keys, expert_ids_turns).reshape((TOKENS_B, TOPK))
    route_weight = jnp.clip(0.2 + 0.8 * jax.random.uniform(seeds[7], (TOKENS_B, TOPK), jnp.float32) ** block_levels(seeds[7], (TOKENS_B, TOPK), ((0, 16),), -0.2, 0.2), 0.2, 1.0)
    gate_weight = centred(seeds[8], (EXPERTS, D, H_E), D ** -0.5, 0.125, ((0, 16), (2, 16)))
    up_weight = centred(seeds[9], (EXPERTS, D, H_E), D ** -0.5, 0.125, ((0, 16), (2, 16)))
    down_weight = centred(seeds[10], (EXPERTS, H_E, D), H_E ** -0.5, 0.0625, ((0, 16), (1, 16)))
    output_gain = jnp.clip(1.0 + 0.18 * jax.random.normal(seeds[11], (D,), jnp.float32), 0.1, 1.9)
    return {"queries": queries, "keys": keys, "values": values, "query_gain": query_gain, "key_gain": key_gain, "moe_input": moe_input, "expert_ids": expert_ids, "route_weight": route_weight, "gate_weight": gate_weight, "up_weight": up_weight, "down_weight": down_weight, "output_gain": output_gain}


rope_theta = 10000.0
rms_epsilon = 1e-06
norm_epsilon = 1e-05
residual_scale = 1.4142135623730951

def unit_heads(heads, gain_vector):
    squares = lax.optimization_barrier(jnp.mean(heads * heads, axis=-1, keepdims=True))
    return heads * lax.rsqrt(squares + rms_epsilon) * gain_vector

def rotate_grid(heads, first_position, grid_width):
    head_size = heads.shape[-1]
    pair_count = head_size // 4
    position = first_position + jnp.arange(heads.shape[1], dtype=jnp.int32)
    grid_row = (position // grid_width).astype(jnp.float32)
    grid_col = (position % grid_width).astype(jnp.float32)
    inverse = rope_theta ** (-jnp.arange(pair_count, dtype=jnp.float32) / pair_count)
    angles = jnp.concatenate([grid_row[:, None] * inverse, grid_col[:, None] * inverse], axis=-1)
    cosines = jnp.cos(angles)
    sines = jnp.sin(angles)
    half_size = head_size // 2
    first_half = heads[..., :half_size]
    second_half = heads[..., half_size:]
    return jnp.concatenate([first_half * cosines - second_half * sines, second_half * cosines + first_half * sines], axis=-1)

def place_rank(choices, expert_count):
    matches = (choices[..., None] == jnp.arange(expert_count, dtype=jnp.int32)).astype(jnp.int32)
    earlier = jnp.cumsum(matches, axis=1) - matches
    return lax.optimization_barrier(jnp.sum(earlier * matches, axis=-1)).astype(jnp.int32)

def attention(queries, keys, values, query_gain, key_gain):
    length = queries.shape[0]
    query_heads = queries.reshape(length, QH, HD).transpose(1, 0, 2).astype(jnp.float32)
    rotated_queries = rotate_grid(unit_heads(query_heads, query_gain), 0, GRID_W).astype(jnp.bfloat16)
    key_heads = keys.reshape(length, KV, HD).transpose(1, 0, 2).astype(jnp.float32)
    rotated_keys = rotate_grid(unit_heads(key_heads, key_gain), 0, GRID_W).astype(jnp.bfloat16)
    value_heads = values.reshape(length, KV, HD).transpose(1, 0, 2)
    query_block = math.gcd(length, 1024)
    group_size = QH // KV
    score_scale = HD ** (-0.5)

    def one_head(head_index):
        key_rows = lax.dynamic_index_in_dim(rotated_keys, head_index // group_size, 0, keepdims=False)
        value_rows = lax.dynamic_index_in_dim(value_heads, head_index // group_size, 0, keepdims=False)
        query_rows = lax.dynamic_index_in_dim(rotated_queries, head_index, 0, keepdims=False)

        def one_block(query_part):
            scores = jnp.dot(query_part, key_rows.T, preferred_element_type=jnp.float32) * score_scale
            row_max = lax.optimization_barrier(jnp.max(scores, axis=-1, keepdims=True))
            weights = jnp.exp(scores - row_max)
            totals = lax.optimization_barrier(jnp.sum(weights, axis=-1, keepdims=True))
            summed = jnp.dot(weights.astype(jnp.bfloat16), value_rows, preferred_element_type=jnp.float32)
            return (summed / totals).astype(jnp.bfloat16)
        blocks = query_rows.reshape(length // query_block, query_block, HD)
        return lax.map(one_block, blocks).reshape(length, HD)
    attended = lax.map(one_head, jnp.arange(QH, dtype=jnp.int32))
    return attended.transpose(1, 0, 2).reshape(length, QH * HD)

def run_expert(operands):
    expert_rows, gate_matrix, up_matrix, down_matrix = operands
    gate_part = jnp.dot(expert_rows, gate_matrix, preferred_element_type=jnp.float32)
    up_part = jnp.dot(expert_rows, up_matrix, preferred_element_type=jnp.float32)
    hidden = (jax.nn.silu(gate_part) * up_part).astype(jnp.bfloat16)
    group_width = hidden.shape[1] // N_TP
    hidden_groups = hidden.reshape(hidden.shape[0], N_TP, group_width).transpose(1, 0, 2)
    down_groups = down_matrix.reshape(N_TP, group_width, down_matrix.shape[1])

    def add_group(running, operand_pair):
        hidden_part, down_part = operand_pair
        partial_sum = jnp.dot(hidden_part, down_part, preferred_element_type=jnp.float32)
        rounded = lax.optimization_barrier(partial_sum.astype(jnp.bfloat16))
        return (running + rounded.astype(jnp.float32), None)
    start_sum = jnp.zeros((hidden.shape[0], down_matrix.shape[1]), jnp.float32)
    summed, ignored = lax.scan(add_group, start_sum, (hidden_groups, down_groups))
    return summed.astype(jnp.bfloat16)

def layer_scale(mixed, gain_vector):
    average = lax.optimization_barrier(jnp.mean(mixed, axis=-1, keepdims=True))
    centered = mixed - average
    variance = lax.optimization_barrier(jnp.mean(centered * centered, axis=-1, keepdims=True))
    return (centered * lax.rsqrt(variance + norm_epsilon) * gain_vector).astype(jnp.bfloat16)

def experts_layer(moe_input, expert_ids, route_weight, gate_weight, up_weight, down_weight, output_gain):
    top_count = expert_ids.shape[1]
    block_count = N_EP * N_TP
    choices = expert_ids.reshape(block_count, TOK_DEV * top_count)
    ranks = place_rank(choices, EXPERTS)
    expert_span = block_count * CAP
    targets = choices * expert_span + jnp.arange(block_count, dtype=jnp.int32)[:, None] * CAP + ranks
    tokens_from = jnp.arange(block_count * TOK_DEV * top_count, dtype=jnp.int32) // top_count
    sources = jnp.full((EXPERTS * expert_span,), block_count * TOK_DEV, jnp.int32).at[targets.reshape(-1)].set(tokens_from)
    gathered = jnp.take(moe_input, sources, axis=0, mode='fill', fill_value=0).reshape(EXPERTS, expert_span, D)
    outputs = lax.map(run_expert, (gathered, gate_weight, up_weight, down_weight))
    picked = jnp.take(outputs.reshape(EXPERTS * expert_span, D), targets.reshape(-1), axis=0)
    picked = picked.reshape(block_count * TOK_DEV, top_count, D).astype(jnp.float32)
    mixed = residual_scale * moe_input.astype(jnp.float32) + lax.optimization_barrier(jnp.sum(route_weight[:, :, None] * picked, axis=1))
    return layer_scale(mixed, output_gain)

def reference(queries, keys, values, query_gain, key_gain, moe_input, expert_ids, route_weight, gate_weight, up_weight, down_weight, output_gain):
    attended = attention(queries, keys, values, query_gain, key_gain)
    moe_output = experts_layer(moe_input, expert_ids, route_weight, gate_weight, up_weight, down_weight, output_gain)
    return (attended, moe_output)
```

```python
import functools
import math

import jax
import jax.numpy as jnp
from jax import lax
from jax.experimental import pallas as pl
from jax.experimental.pallas import tpu as pltpu
from jax.sharding import PartitionSpec as P

QH = 16
KV = 4
GRID_W = 64
MESH = pl.DeviceIdType.MESH
BF16 = jnp.bfloat16
F32 = jnp.float32

rope_theta = 10000.0
rms_epsilon = 1e-06
norm_epsilon = 1e-05
residual_scale = 1.4142135623730951

PAD = 8
NCHUNK = 4


def unit_heads(heads, gain_vector):
    squares = jnp.mean(heads * heads, axis=-1, keepdims=True)
    return heads * lax.rsqrt(squares + rms_epsilon) * gain_vector


def rotate_grid(heads, first_position, grid_width):
    head_size = heads.shape[-1]
    pair_count = head_size // 4
    position = first_position + jnp.arange(heads.shape[0], dtype=jnp.int32)
    grid_row = (position // grid_width).astype(F32)
    grid_col = (position % grid_width).astype(F32)
    inverse = rope_theta ** (-jnp.arange(pair_count, dtype=F32) / pair_count)
    angles = jnp.concatenate([grid_row[:, None] * inverse, grid_col[:, None] * inverse], axis=-1)
    cosines = jnp.cos(angles)
    sines = jnp.sin(angles)
    half_size = head_size // 2
    first_half = heads[..., :half_size]
    second_half = heads[..., half_size:]
    return jnp.concatenate(
        [first_half * cosines - second_half * sines, second_half * cosines + first_half * sines],
        axis=-1,
    )


def attention_kernel(scale, kb, width, qt_ref, kv_ref, o_ref, vt, s0, s1):
    length = kv_ref.shape[0]
    nk = length // kb
    hd = o_ref.shape[1]
    tb = 1024

    def turn(j, carry):
        rows = pl.ds(pl.multiple_of(j * tb, tb), tb)
        vt[0:hd, rows] = kv_ref[rows, :].T[hd : 2 * hd]
        vt[hd : hd + 16, rows] = jnp.ones((16, tb), BF16)
        return carry

    lax.fori_loop(0, length // tb, turn, 0)
    for first in range(0, qt_ref.shape[1], width):

        def score(j, sref):
            rows = pl.ds(pl.multiple_of(j * kb, kb), kb)
            s = jnp.dot(
                kv_ref[rows, :], qt_ref[:, first : first + width], preferred_element_type=F32
            )
            sref[...] = s
            return jnp.max(s, axis=0, keepdims=True)

        def absorb(j, sref, state, top):
            m, acc = state
            rows = pl.ds(pl.multiple_of(j * kb, kb), kb)
            new = jnp.maximum(m, top)
            p = jnp.exp2((sref[...] - new) * scale).astype(BF16)
            shrink = jnp.exp2((m - new) * scale)
            return new, acc * shrink + jnp.dot(vt[:, rows], p, preferred_element_type=F32)

        def pair(i, carry):
            state, top0 = carry
            top1 = score(2 * i + 1, s1)
            state = absorb(2 * i, s0, state, top0)
            top2 = score(jnp.minimum(2 * i + 2, nk - 1), s0)
            state = absorb(2 * i + 1, s1, state, top1)
            return state, top2

        init = (jnp.full((1, width), -jnp.inf, F32), jnp.zeros((hd + 16, width), F32))
        (m, acc), _ = lax.fori_loop(0, nk // 2, pair, (init, score(0, s0)))
        o_ref[first : first + width, :] = (acc[0:hd] / acc[hd : hd + 1]).astype(BF16).T


def attend(qt, kv, head_size):
    length, rows = kv.shape[0], qt.shape[1]
    kb, width = 1024, 512
    return pl.pallas_call(
        functools.partial(attention_kernel, head_size**-0.5 * math.log2(math.e), kb, width),
        out_shape=jax.ShapeDtypeStruct((rows, head_size), BF16),
        in_specs=[pl.BlockSpec(memory_space=pltpu.VMEM)] * 2,
        out_specs=pl.BlockSpec(memory_space=pltpu.VMEM),
        scratch_shapes=[
            pltpu.VMEM((head_size + 16, length), BF16),
            pltpu.VMEM((kb, width), F32),
            pltpu.VMEM((kb, width), F32),
        ],
        compiler_params=pltpu.CompilerParams(vmem_limit_bytes=40 * 1024 * 1024),
        cost_estimate=pl.CostEstimate(
            flops=4 * length * rows * 128,
            bytes_accessed=4 * length * 128,
            transcendentals=length * rows,
        ),
    )(qt, kv)


def experts_kernel(
    n_ep,
    n_z,
    slots_row,
    slots_col,
    route,
    x_ref,
    gain_ref,
    gate_hbm,
    up_hbm,
    down_hbm,
    out_ref,
    gate,
    up,
    down,
    outgoing,
    dispatched,
    blocks,
    parts,
    partner_parts,
    ring_in,
    returned,
    load_sem,
    disp_send,
    disp_recv,
    gath_send,
    gath_recv,
    pair_send,
    pair_recv,
    part_send,
    part_recv,
    red_send,
    red_recv,
    ret_send,
    ret_recv,
):
    e = lax.axis_index("ep")
    t = lax.axis_index("tp")
    z = t // 2
    c = t % 2
    way = 1 - 2 * c
    tokens, width = x_ref.shape
    rows = blocks.shape[2]
    cap = rows // n_ep
    slots = n_ep * PAD
    cw = width // NCHUNK
    last = n_z - 1

    def at_z(distance):
        return lax.rem(z + distance + 2 * n_z, n_z)

    ring_to = (e, at_z(way) * 2 + c)
    partner = (e, z * 2 + 1 - c)

    loads = [
        pltpu.make_async_copy(src, dst, load_sem.at[i])
        for i, (src, dst) in enumerate(((gate_hbm, gate), (up_hbm, up), (down_hbm, down)))
    ]
    for load in loads:
        load.start()

    barrier = pltpu.get_barrier_semaphore()
    for d in range(1, n_ep):
        pl.semaphore_signal(
            barrier, inc=1, device_id=(lax.rem(e + d, n_ep), t), device_id_type=MESH
        )
    for peer in ((e, at_z(1) * 2 + c), (e, at_z(-1) * 2 + c), partner):
        pl.semaphore_signal(barrier, inc=1, device_id=peer, device_id_type=MESH)

    slot = lax.broadcasted_iota(jnp.int32, (slots, tokens), 0)
    pick = jnp.where((slot == slots_row[0:1, :]) | (slot == slots_row[1:2, :]), 1.0, 0.0)
    outgoing[...] = (
        jnp.dot(pick.astype(BF16), x_ref[...], preferred_element_type=F32)
        .astype(BF16)
        .reshape(n_ep, PAD, width)
    )
    dispatched[pl.ds(e, 1)] = outgoing[pl.ds(e, 1)]
    pl.semaphore_wait(barrier, n_ep - 1 + 3)

    def exchange(src, dst, send, recv, d):
        to = lax.rem(e + d, n_ep)
        return pltpu.make_async_remote_copy(
            src_ref=src.at[to],
            dst_ref=dst.at[e],
            send_sem=send.at[d],
            recv_sem=recv.at[d],
            device_id=(to, t),
            device_id_type=MESH,
        )

    for d in range(1, n_ep):
        exchange(outgoing, dispatched, disp_send, disp_recv, d).start()
    for d in range(1, n_ep):
        exchange(outgoing, dispatched, disp_send, disp_recv, d).wait_recv()

    r_i = lax.broadcasted_iota(jnp.int32, (rows, slots), 0)
    s_i = lax.broadcasted_iota(jnp.int32, (rows, slots), 1)
    squeeze = jnp.where(s_i == (r_i // cap) * PAD + r_i % cap, 1.0, 0.0).astype(BF16)
    blocks[pl.ds(c, 1), pl.ds(z, 1)] = (
        jnp.dot(squeeze, dispatched[...].reshape(slots, width), preferred_element_type=F32)
        .astype(BF16)
        .reshape(1, 1, rows, width)
    )

    def gather_copy(s, k):
        ref = blocks.at[c, at_z(-way * s), :, pl.ds(k * cw, cw)]
        return pltpu.make_async_remote_copy(
            src_ref=ref,
            dst_ref=ref,
            send_sem=gath_send.at[s * NCHUNK + k],
            recv_sem=gath_recv.at[s * NCHUNK + k],
            device_id=ring_to,
            device_id_type=MESH,
        )

    def pair_copy(s):
        ref = blocks.at[c, at_z(-way * s)]
        return pltpu.make_async_remote_copy(
            src_ref=ref,
            dst_ref=ref,
            send_sem=pair_send.at[s],
            recv_sem=pair_recv.at[s],
            device_id=partner,
            device_id_type=MESH,
        )

    def part_copy(s):
        return pltpu.make_async_remote_copy(
            src_ref=parts.at[1 - c, at_z(way * s)],
            dst_ref=partner_parts.at[at_z(way * s)],
            send_sem=part_send.at[s],
            recv_sem=part_recv.at[s],
            device_id=partner,
            device_id_type=MESH,
        )

    def reduce_copy(s, k):
        cols = pl.ds(k * cw, cw)
        return pltpu.make_async_remote_copy(
            src_ref=parts.at[c, at_z(-way * (s + 1)), :, cols],
            dst_ref=ring_in.at[s, :, cols],
            send_sem=red_send.at[s * NCHUNK + k],
            recv_sem=red_recv.at[s * NCHUNK + k],
            device_id=ring_to,
            device_id_type=MESH,
        )

    def feed(ring, zi):
        xb = blocks[pl.ds(ring, 1), pl.ds(zi, 1)].reshape(rows, width)
        g = jnp.dot(xb, gate[...], preferred_element_type=F32)
        u = jnp.dot(xb, up[...], preferred_element_type=F32)
        hidden = ((g / (1.0 + jnp.exp(-g))) * u).astype(BF16)
        part = jnp.dot(hidden, down[...], preferred_element_type=F32).astype(BF16)
        parts[pl.ds(ring, 1), pl.ds(zi, 1)] = part.reshape(1, 1, rows, width)

    def feed_own(s):
        feed(c, at_z(-way * s))

    def feed_partner(s):
        pair_copy(s).wait_recv()
        feed(1 - c, at_z(way * s))
        part_copy(s).start()

    for k in range(NCHUNK):
        gather_copy(0, k).start()
    pair_copy(0).start()
    for load in loads:
        load.wait()

    def gather_step(s, carry):
        def forward(k):
            gather_copy(s, k).wait_recv()

            @pl.when(s < last - 1)
            def _():
                gather_copy(s + 1, k).start()

        forward(0)
        forward(1)
        feed_own(s)
        forward(2)
        feed_partner(s)
        forward(3)
        pair_copy(s + 1).start()
        return carry

    lax.fori_loop(0, last, gather_step, 0)

    def reduce_step(s, carry):
        b = at_z(-way * (s + 1))
        part_copy(s + 1).wait_recv()
        for k in range(NCHUNK):
            cols = pl.ds(k * cw, cw)
            value = parts[pl.ds(c, 1), pl.ds(b, 1), :, cols].astype(F32).reshape(rows, cw)
            value += partner_parts[pl.ds(b, 1), :, cols].astype(F32).reshape(rows, cw)
            reduce_copy(s - 1, k).wait_recv()
            value += ring_in[pl.ds(s - 1, 1), :, cols].astype(F32).reshape(rows, cw)
            parts[pl.ds(c, 1), pl.ds(b, 1), :, cols] = value.astype(BF16).reshape(1, 1, rows, cw)
            reduce_copy(s, k).start()
        return carry

    b = at_z(-way)
    part_copy(1).wait_recv()
    for k in range(NCHUNK):
        cols = pl.ds(k * cw, cw)
        value = parts[pl.ds(c, 1), pl.ds(b, 1), :, cols].astype(F32).reshape(rows, cw)
        value += partner_parts[pl.ds(b, 1), :, cols].astype(F32).reshape(rows, cw)
        parts[pl.ds(c, 1), pl.ds(b, 1), :, cols] = value.astype(BF16).reshape(1, 1, rows, cw)
        reduce_copy(0, k).start()
    feed_partner(last)
    feed_own(last)
    lax.fori_loop(1, last, reduce_step, 0)

    part_copy(0).wait_recv()
    total = parts[pl.ds(c, 1), pl.ds(z, 1)].astype(F32).reshape(rows, width)
    total += partner_parts[pl.ds(z, 1)].astype(F32).reshape(rows, width)
    for k in range(NCHUNK):
        reduce_copy(last - 1, k).wait_recv()
    total += ring_in[last - 1].astype(F32)
    r_j = lax.broadcasted_iota(jnp.int32, (slots, rows), 1)
    s_j = lax.broadcasted_iota(jnp.int32, (slots, rows), 0)
    spread = jnp.where(s_j == (r_j // cap) * PAD + r_j % cap, 1.0, 0.0).astype(BF16)
    for d in range(1, n_ep):
        exchange(outgoing, dispatched, disp_send, disp_recv, d).wait_send()
    outgoing[...] = (
        jnp.dot(spread, total.astype(BF16), preferred_element_type=F32)
        .astype(BF16)
        .reshape(n_ep, PAD, width)
    )
    returned[pl.ds(e, 1)] = outgoing[pl.ds(e, 1)]
    for d in range(1, n_ep):
        exchange(outgoing, returned, ret_send, ret_recv, d).start()

    for s in range(n_z):
        pair_copy(s).wait_send()
        part_copy(s).wait_send()
    for s in range(last):
        for k in range(NCHUNK):
            gather_copy(s, k).wait_send()
            reduce_copy(s, k).wait_send()
    mixed = residual_scale * x_ref[...].astype(F32)
    for d in range(1, n_ep):
        exchange(outgoing, returned, ret_send, ret_recv, d).wait_recv()
    back = returned[...].reshape(slots, width)
    lane = lax.broadcasted_iota(jnp.int32, (tokens, slots), 1)
    both = None
    for k in range(slots_col.shape[1]):
        one = jnp.where(lane == slots_col[:, k : k + 1], 1.0, 0.0).astype(BF16)
        term = route[:, k : k + 1] * jnp.dot(one, back, preferred_element_type=F32)
        both = term if both is None else both + term
    mixed += both
    average = jnp.mean(mixed, axis=-1, keepdims=True)
    centered = mixed - average
    variance = jnp.mean(centered * centered, axis=-1, keepdims=True)
    out_ref[...] = (centered * lax.rsqrt(variance + norm_epsilon) * gain_ref[...]).astype(BF16)
    for d in range(1, n_ep):
        exchange(outgoing, returned, ret_send, ret_recv, d).wait_send()


def experts(slots_row, slots_col, route, x, gain, gate, up, down, n_ep, n_z, cap):
    tokens, width = x.shape
    hidden = gate.shape[1]
    rows = n_ep * cap
    vmem = pl.BlockSpec(memory_space=pltpu.VMEM)
    hbm = pl.BlockSpec(memory_space=pl.ANY)
    dma = pltpu.SemaphoreType.DMA
    hops = (n_z - 1) * NCHUNK
    return pl.pallas_call(
        functools.partial(experts_kernel, n_ep, n_z),
        out_shape=jax.ShapeDtypeStruct((tokens, width), BF16),
        in_specs=[vmem] * 5 + [hbm] * 3,
        out_specs=vmem,
        scratch_shapes=[
            pltpu.VMEM((width, hidden), BF16),
            pltpu.VMEM((width, hidden), BF16),
            pltpu.VMEM((hidden, width), BF16),
            pltpu.VMEM((n_ep, PAD, width), BF16),
            pltpu.VMEM((n_ep, PAD, width), BF16),
            pltpu.VMEM((2, n_z, rows, width), BF16),
            pltpu.VMEM((2, n_z, rows, width), BF16),
            pltpu.VMEM((n_z, rows, width), BF16),
            pltpu.VMEM((n_z - 1, rows, width), BF16),
            pltpu.VMEM((n_ep, PAD, width), BF16),
            dma((3,)),
            dma((n_ep,)),
            dma((n_ep,)),
            dma((hops,)),
            dma((hops,)),
            dma((n_z,)),
            dma((n_z,)),
            dma((n_z,)),
            dma((n_z,)),
            dma((hops,)),
            dma((hops,)),
            dma((n_ep,)),
            dma((n_ep,)),
        ],
        compiler_params=pltpu.CompilerParams(
            collective_id=0, has_side_effects=True, vmem_limit_bytes=50 * 1024 * 1024
        ),
        cost_estimate=pl.CostEstimate(
            flops=12 * n_z * rows * width * hidden,
            bytes_accessed=6 * width * hidden,
            transcendentals=0,
        ),
    )(slots_row, slots_col, route, x, gain, gate, up, down)


def shards(
    queries,
    keys,
    values,
    query_gain,
    key_gain,
    moe_input,
    expert_ids,
    route_weight,
    gate_weight,
    up_weight,
    down_weight,
    output_gain,
):
    seg_rows = queries.shape[0]
    head_size = query_gain.shape[0]
    tp = lax.axis_index("tp")
    offset = lax.axis_index("ep") * seg_rows
    key_head = tp // (QH // KV)
    key_cols = lax.dynamic_slice_in_dim(keys, key_head * head_size, head_size, 1)
    value_cols = lax.dynamic_slice_in_dim(values, key_head * head_size, head_size, 1)
    rotated_queries = rotate_grid(
        unit_heads(queries.astype(F32), query_gain), offset, GRID_W
    ).astype(BF16)
    rotated_keys = rotate_grid(unit_heads(key_cols.astype(F32), key_gain), offset, GRID_W).astype(
        BF16
    )
    kv = lax.all_gather(
        jnp.concatenate([rotated_keys, value_cols], axis=1), "ep", axis=0, tiled=True
    )
    qt = jnp.concatenate(
        [rotated_queries.T, jnp.zeros((head_size, seg_rows), BF16)], axis=0
    )

    tok_rows = moe_input.shape[0]
    top_count = expert_ids.shape[1]
    n_ep = lax.axis_size("ep")
    n_tp = lax.axis_size("tp")
    cap = max(2, tok_rows * top_count * 5 // (4 * n_ep))
    own_ids = lax.dynamic_slice_in_dim(expert_ids, tp * tok_rows, tok_rows, 0)
    own_route = lax.dynamic_slice_in_dim(route_weight, tp * tok_rows, tok_rows, 0)
    flat = own_ids.reshape(-1)
    order = jnp.arange(flat.shape[0], dtype=jnp.int32)
    earlier = (flat[:, None] == flat[None, :]) & (order[None, :] < order[:, None])
    rank = jnp.sum(earlier.astype(jnp.int32), axis=1)
    slots_col = (flat * PAD + rank).reshape(tok_rows, top_count)
    moe_output = experts(
        slots_col.T,
        slots_col,
        own_route,
        moe_input,
        output_gain[None, :],
        gate_weight[0],
        up_weight[0],
        down_weight[0],
        n_ep,
        n_tp // 2,
        cap,
    )
    attended = attend(qt, kv, head_size)
    return (attended, moe_output)


def solution(mesh):
    return jax.shard_map(
        shards,
        mesh=mesh,
        in_specs=(
            P("ep", "tp"),
            P("ep", None),
            P("ep", None),
            P(),
            P(),
            P(("ep", "tp"), None),
            P("ep", None),
            P("ep", None),
            P("ep", None, "tp"),
            P("ep", None, "tp"),
            P("ep", "tp", None),
            P(),
        ),
        out_specs=(P("ep", "tp"), P(("ep", "tp"), None)),
        check_vma=False,
    )
```

```python
import functools
import math

import jax
import jax.numpy as jnp
import numpy as np
from jax import lax
from jax.experimental import pallas as pl
from jax.experimental.pallas import tpu as pltpu
from jax.sharding import PartitionSpec as P

QH = 16
KV = 4
GRID_W = 64
MESH = pl.DeviceIdType.MESH
BF16 = jnp.bfloat16
F32 = jnp.float32

rope_theta = 10000.0
rms_epsilon = 1e-06
norm_epsilon = 1e-05
residual_scale = 1.4142135623730951

PAD = 8
NCHUNK = 4
Q_WIDTH = 512
K_BLOCK = 512
PIECES = (0, 2, 3, 5, 6)
LANES = 128
VMEM_LIMIT = 58 * 1024 * 1024
KV_GROUP = 3
KV_FROM = 4


def rotated(heads_t, gain_col, cosines, sines):
    squares = jnp.mean(heads_t * heads_t, axis=0, keepdims=True)
    unit = heads_t * lax.rsqrt(squares + rms_epsilon) * gain_col
    half = heads_t.shape[0] // 2
    a, b = unit[0:half], unit[half:]
    return jnp.concatenate([a * cosines - b * sines, b * cosines + a * sines], axis=0)


def layer_kernel(
    n_ep,
    n_z,
    group,
    ids_ref,
    route_ref,
    x_ref,
    gain_ref,
    qt_ref,
    q_gain,
    k_gain,
    keys_hbm,
    values_hbm,
    gate_hbm,
    up_hbm,
    down_hbm,
    att_ref,
    out_ref,
    gate_t,
    up_t,
    gate,
    up,
    down,
    key_cols,
    value_cols,
    kv,
    vt,
    qt,
    s0,
    s1,
    top,
    peak,
    acc,
    outgoing,
    dispatched,
    blocks,
    parts,
    partner_parts,
    ring_in,
    returned,
    mixed,
    meta,
    load_sem,
    disp_send,
    disp_recv,
    gath_send,
    gath_recv,
    pair_send,
    pair_recv,
    part_send,
    part_recv,
    red_send,
    red_recv,
    ret_send,
    ret_recv,
    kv_send,
    kv_recv,
    kvp_send,
    kvp_recv,
):
    e = lax.axis_index("ep")
    t = lax.axis_index("tp")
    z = t // 2
    c = t % 2
    way = 1 - 2 * c
    tokens, width = x_ref.shape
    rows = blocks.shape[2]
    cap = rows // n_ep
    slots = n_ep * PAD
    cw = width // NCHUNK
    last = n_z - 1

    def at_z(distance):
        return lax.rem(z + distance + 2 * n_z, n_z)

    ring_to = (e, at_z(way) * 2 + c)
    partner = (e, z * 2 + 1 - c)

    hd = q_gain.shape[1]
    seg = qt_ref.shape[1]
    key_head = t // group
    head_cols = pl.ds(pl.multiple_of(key_head // 2 * (2 * hd), 2 * hd), 2 * hd)
    loads = [
        pltpu.make_async_copy(src, dst, load_sem.at[i])
        for i, (src, dst) in enumerate(
            (
                (keys_hbm.at[:, head_cols], key_cols),
                (values_hbm.at[:, head_cols], value_cols),
                (gate_hbm, gate_t),
                (up_hbm, up_t),
                (down_hbm, down),
            )
        )
    ]
    for load in loads:
        load.start()

    barrier = pltpu.get_barrier_semaphore()
    for d in range(1, n_ep):
        pl.semaphore_signal(
            barrier, inc=1, device_id=(lax.rem(e + d, n_ep), t), device_id_type=MESH
        )
    for peer in ((e, at_z(1) * 2 + c), (e, at_z(-1) * 2 + c), partner):
        pl.semaphore_signal(barrier, inc=1, device_id=peer, device_id_type=MESH)

    top_count = ids_ref.shape[0]
    column_tokens = ids_ref.shape[1]
    meta[...] = jnp.zeros(meta.shape, F32)
    meta[0:top_count, :] = ids_ref[...].astype(F32)
    meta[top_count : 2 * top_count, :] = route_ref[...]
    own = pltpu.roll(
        meta[...], lax.rem(column_tokens - t * tokens, column_tokens), axis=1
    )[:, 0:LANES]
    own_t = own.T
    sub_i = lax.broadcasted_iota(jnp.int32, (LANES, LANES), 0)
    lane_i = lax.broadcasted_iota(jnp.int32, (LANES, LANES), 1)
    slot_rows, slot_cols = [], []
    for k in range(top_count):
        row, col = own[k : k + 1, :], own_t[:, k : k + 1]
        hit_r = sum(jnp.where(own_t[:, j : j + 1] == row, 1.0, 0.0) for j in range(top_count))
        hit_c = sum(jnp.where(own[j : j + 1, :] == col, 1.0, 0.0) for j in range(top_count))
        rank_r = jnp.sum(jnp.where(sub_i < lane_i, hit_r, 0.0), axis=0, keepdims=True)
        rank_c = jnp.sum(jnp.where(lane_i < sub_i, hit_c, 0.0), axis=1, keepdims=True)
        slot_rows.append((row * PAD + rank_r)[:, 0:tokens])
        slot_cols.append((col * PAD + rank_c)[0:tokens, :])

    slot = lax.broadcasted_iota(jnp.int32, (slots, tokens), 0).astype(F32)
    pick = sum(jnp.where(slot == row, 1.0, 0.0) for row in slot_rows)
    outgoing[...] = (
        jnp.dot(pick.astype(BF16), x_ref[...], preferred_element_type=F32)
        .astype(BF16)
        .reshape(n_ep, PAD, width)
    )
    dispatched[pl.ds(e, 1)] = outgoing[pl.ds(e, 1)]
    pl.semaphore_wait(barrier, n_ep - 1 + 3)

    def exchange(src, dst, send, recv, d, k):
        to = lax.rem(e + d, n_ep)
        cols = pl.ds(k * cw, cw)
        return pltpu.make_async_remote_copy(
            src_ref=src.at[to, :, cols],
            dst_ref=dst.at[e, :, cols],
            send_sem=send.at[0],
            recv_sem=recv.at[k],
            device_id=(to, t),
            device_id_type=MESH,
        )

    def each(act):
        def one(d, carry):
            act(d)
            return carry

        lax.fori_loop(1, n_ep, one, 0)

    def dispatch(d, k):
        return exchange(outgoing, dispatched, disp_send, disp_recv, d, k)

    def give_back(d, k):
        return exchange(outgoing, returned, ret_send, ret_recv, d, k)

    def wait_bytes(ref, sem):
        pltpu.make_async_copy(ref, ref, sem).wait()

    def chunk_bytes(ref, k):
        return ref.at[pl.ds(0, n_ep - 1), :, pl.ds(k * cw, cw)]

    for k in range(NCHUNK):
        each(lambda d: dispatch(d, k).start())
    def kv_copy(d):
        rows_c = pl.ds(pl.multiple_of(c * (seg // 2), seg // 2), seg // 2)
        return pltpu.make_async_remote_copy(
            src_ref=kv.at[e, rows_c, :],
            dst_ref=kv.at[e, rows_c, :],
            send_sem=kv_send.at[0],
            recv_sem=kv_recv.at[(d - 1) // KV_GROUP],
            device_id=(lax.rem(e + d, n_ep), t),
            device_id_type=MESH,
        )

    def kv_pair_copy(d):
        rows_c = pl.ds(pl.multiple_of(c * (seg // 2), seg // 2), seg // 2)
        ref = kv.at[lax.rem(e - d + n_ep, n_ep), rows_c, :]
        return pltpu.make_async_remote_copy(
            src_ref=ref,
            dst_ref=ref,
            send_sem=kvp_send.at[0],
            recv_sem=kvp_recv.at[0],
            device_id=partner,
            device_id_type=MESH,
        )

    lane = lax.broadcasted_iota(jnp.int32, (1, seg), 1)
    position = e * seg + lane
    grid_row = (position // GRID_W).astype(F32)
    grid_col = (position % GRID_W).astype(F32)
    quarter = hd // 4
    freq_i = lax.broadcasted_iota(jnp.int32, (quarter, 1), 0)
    inverse = jnp.zeros((quarter, 1), F32)
    for j in range(quarter):
        inverse = jnp.where(freq_i == j, float(np.float32(rope_theta ** (-j / quarter))), inverse)
    angles = jnp.concatenate([inverse * grid_row, inverse * grid_col], axis=0)
    gain_eye = lax.broadcasted_iota(jnp.int32, (hd, hd), 0) == lax.broadcasted_iota(
        jnp.int32, (hd, hd), 1
    )

    def column(row_ref):
        return jnp.sum(jnp.where(gain_eye, row_ref[...], 0.0), axis=1, keepdims=True)

    cosines, sines = jnp.cos(angles), jnp.sin(angles)
    odd = key_head % 2 == 1
    loads[0].wait()
    loads[1].wait()
    keys_t = key_cols[...].T.astype(F32)
    values_t = value_cols[...].T.astype(F32)
    own_k = rotated(jnp.where(odd, keys_t[hd:], keys_t[:hd]), column(k_gain), cosines, sines)
    own_v = jnp.where(odd, values_t[hd:], values_t[:hd])
    kv[pl.ds(e, 1)] = (
        jnp.concatenate([own_k.astype(BF16), own_v.astype(BF16)], axis=0)
        .T.reshape(1, seg, 2 * hd)
    )
    loads[2].wait()
    loads[3].wait()
    step = width // NCHUNK
    for k in range(NCHUNK):
        gate[k * step : (k + 1) * step, :] = gate_t[:, k * step : (k + 1) * step].T
        up[k * step : (k + 1) * step, :] = up_t[:, k * step : (k + 1) * step].T

    def gather_copy(s, k):
        ref = blocks.at[c, at_z(-way * s), :, pl.ds(k * cw, cw)]
        return pltpu.make_async_remote_copy(
            src_ref=ref,
            dst_ref=ref,
            send_sem=gath_send.at[0],
            recv_sem=gath_recv.at[s * NCHUNK + k],
            device_id=ring_to,
            device_id_type=MESH,
        )

    def pair_copy(s):
        ref = blocks.at[c, at_z(-way * s)]
        return pltpu.make_async_remote_copy(
            src_ref=ref,
            dst_ref=ref,
            send_sem=pair_send.at[0],
            recv_sem=pair_recv.at[s],
            device_id=partner,
            device_id_type=MESH,
        )

    def part_copy(s):
        return pltpu.make_async_remote_copy(
            src_ref=parts.at[1 - c, at_z(way * s)],
            dst_ref=partner_parts.at[at_z(way * s)],
            send_sem=part_send.at[0],
            recv_sem=part_recv.at[s],
            device_id=partner,
            device_id_type=MESH,
        )

    def reduce_copy(s, k):
        cols = pl.ds(k * cw, cw)
        return pltpu.make_async_remote_copy(
            src_ref=parts.at[c, at_z(-way * (s + 1)), :, cols],
            dst_ref=ring_in.at[s, :, cols],
            send_sem=red_send.at[0],
            recv_sem=red_recv.at[s * NCHUNK + k],
            device_id=ring_to,
            device_id_type=MESH,
        )

    def feed(ring, zi):
        xb = blocks[pl.ds(ring, 1), pl.ds(zi, 1)].reshape(rows, width)
        g = jnp.dot(xb, gate[...], preferred_element_type=F32)
        u = jnp.dot(xb, up[...], preferred_element_type=F32)
        hidden = ((g / (1.0 + jnp.exp(-g))) * u).astype(BF16)
        part = jnp.dot(hidden, down[...], preferred_element_type=F32).astype(BF16)
        parts[pl.ds(ring, 1), pl.ds(zi, 1)] = part.reshape(1, 1, rows, width)

    def feed_own(s):
        feed(c, at_z(-way * s))

    def feed_partner(s):
        pair_copy(s).wait_recv()
        feed(1 - c, at_z(way * s))
        part_copy(s).start()

    kb = s0.shape[0]
    q_width = s0.shape[1]
    nk = n_ep * seg // kb
    tiles = nk * (seg // q_width)
    score_scale = hd**-0.5 * math.log2(math.e)

    def score(n, sref):
        rows_n = pl.ds(pl.multiple_of(lax.rem(n, nk) * kb, kb), kb)
        flat = kv.reshape(n_ep * seg, 2 * hd)
        q = qt[pl.ds(n // nk, 1)].reshape(2 * hd, q_width)
        sc = jnp.dot(flat[rows_n, :], q, preferred_element_type=F32)
        sref[...] = sc
        return jnp.max(sc, axis=0, keepdims=True)

    def absorb(n, sref, state, best):
        m, total = state
        cols_n = pl.ds(pl.multiple_of(lax.rem(n, nk) * kb, kb), kb)
        new = jnp.maximum(m, best)
        p = jnp.exp2((sref[...] - new) * score_scale).astype(BF16)
        shrink = jnp.exp2((m - new) * score_scale)
        return new, total * shrink + jnp.dot(vt[:, cols_n], p, preferred_element_type=F32)

    def piece(i):
        n = 2 * i
        group_i = pl.ds(n // nk, 1)
        best0 = top[...]
        state = (peak[group_i].reshape(1, q_width), acc[group_i].reshape(hd + 16, q_width))
        best1 = score(n + 1, s1)
        state = absorb(n, s0, state, best0)
        best2 = score(jnp.minimum(n + 2, tiles - 1), s0)
        m, total = absorb(n + 1, s1, state, best1)
        top[...] = best2
        peak[group_i] = m.reshape(1, 1, q_width)
        acc[group_i] = total.reshape(1, hd + 16, q_width)

    r_i = lax.broadcasted_iota(jnp.int32, (rows, slots), 0)
    s_i = lax.broadcasted_iota(jnp.int32, (rows, slots), 1)
    squeeze = jnp.where(s_i == (r_i // cap) * PAD + r_i % cap, 1.0, 0.0).astype(BF16)
    for k in range(NCHUNK):
        cols = pl.ds(k * cw, cw)
        wait_bytes(chunk_bytes(dispatched, k), disp_recv.at[k])
        came = dispatched[:, :, cols].reshape(slots, cw)
        blocks[pl.ds(c, 1), pl.ds(z, 1), :, cols] = (
            jnp.dot(squeeze, came, preferred_element_type=F32)
            .astype(BF16)
            .reshape(1, 1, rows, cw)
        )
        gather_copy(0, k).start()
    pair_copy(0).start()
    each(lambda d: kv_copy(d).start())
    own_q = rotated(qt_ref[...].astype(F32), column(q_gain), cosines, sines).astype(BF16)
    for g in range(seg // q_width):
        qt[g, 0:hd, :] = own_q[:, g * q_width : (g + 1) * q_width]
        qt[g, hd : 2 * hd, :] = jnp.zeros((hd, q_width), BF16)
    peak[...] = jnp.full(peak.shape, -jnp.inf, F32)
    acc[...] = jnp.zeros(acc.shape, F32)
    loads[4].wait()

    def half_bytes(n):
        return kv.at[pl.ds(0, n), pl.ds(0, seg // 2), :]

    def kv_forward(g):
        wait_bytes(half_bytes(KV_GROUP), kv_recv.at[g])
        for i in range(KV_GROUP):
            kv_pair_copy(g * KV_GROUP + 1 + i).start()

    def gather_step(s, carry):
        def forward(k):
            gather_copy(s, k).wait_recv()
            gather_copy(s + 1, k).start()

        forward(0)
        forward(1)
        feed_own(s)
        forward(2)

        @pl.when(s >= KV_FROM)
        def _():
            kv_forward(s - KV_FROM)

        feed_partner(s)
        forward(3)
        pair_copy(s + 1).start()
        return carry

    lax.fori_loop(0, last - 1, gather_step, 0)

    def first_hop(k):
        b = at_z(-way)
        cols = pl.ds(k * cw, cw)
        value = parts[pl.ds(c, 1), pl.ds(b, 1), :, cols].astype(F32).reshape(rows, cw)
        value += partner_parts[pl.ds(b, 1), :, cols].astype(F32).reshape(rows, cw)
        parts[pl.ds(c, 1), pl.ds(b, 1), :, cols] = value.astype(BF16).reshape(1, 1, rows, cw)
        reduce_copy(0, k).start()

    part_copy(1).wait_recv()
    for k in range(NCHUNK):
        first_hop(k)
    for g in range(last - 1 - KV_FROM, (n_ep - 1) // KV_GROUP):
        kv_forward(g)
    feed_own(last - 1)
    feed_partner(last - 1)
    for k in range(NCHUNK):
        gather_copy(last - 1, k).wait_recv()
    pair_copy(last).start()
    feed_own(last)
    feed_partner(last)

    def turn(j, carry):
        cols = pl.ds(pl.multiple_of(j * seg, seg), seg)
        vt[0:hd, cols] = kv[pl.ds(j, 1)].reshape(seg, 2 * hd).T[hd : 2 * hd]
        vt[hd : hd + 16, cols] = jnp.ones((16, seg), BF16)
        return carry

    def reduce_step(s, carry):
        b = at_z(-way * (s + 1))
        part_copy(s + 1).wait_recv()
        for k in range(NCHUNK):
            cols = pl.ds(k * cw, cw)
            value = parts[pl.ds(c, 1), pl.ds(b, 1), :, cols].astype(F32).reshape(rows, cw)
            value += partner_parts[pl.ds(b, 1), :, cols].astype(F32).reshape(rows, cw)
            reduce_copy(s - 1, k).wait_recv()
            value += ring_in[pl.ds(s - 1, 1), :, cols].astype(F32).reshape(rows, cw)
            parts[pl.ds(c, 1), pl.ds(b, 1), :, cols] = value.astype(BF16).reshape(1, 1, rows, cw)
            reduce_copy(s, k).start()

            @pl.when(s > 1)
            def _():
                for i in range(PIECES[k], PIECES[k + 1]):
                    piece((s - 2) * PIECES[-1] + i)

        @pl.when(s == 1)
        def _():
            wait_bytes(half_bytes(n_ep - 1), kvp_recv.at[0])
            lax.fori_loop(0, n_ep, turn, 0)
            top[...] = score(0, s0)

        return carry

    lax.fori_loop(1, last, reduce_step, 0)

    r_j = lax.broadcasted_iota(jnp.int32, (slots, rows), 1)
    s_j = lax.broadcasted_iota(jnp.int32, (slots, rows), 0)
    spread = jnp.where(s_j == (r_j // cap) * PAD + r_j % cap, 1.0, 0.0).astype(BF16)
    wait_bytes(outgoing.at[pl.ds(0, n_ep - 1)], disp_send.at[0])
    part_copy(0).wait_recv()
    done = (last - 2) * PIECES[-1]
    extra = -(-(tiles // 2 - done) // NCHUNK)
    for k in range(NCHUNK):
        cols = pl.ds(k * cw, cw)
        value = parts[pl.ds(c, 1), pl.ds(z, 1), :, cols].astype(F32).reshape(rows, cw)
        value += partner_parts[pl.ds(z, 1), :, cols].astype(F32).reshape(rows, cw)
        reduce_copy(last - 1, k).wait_recv()
        value += ring_in[last - 1, :, cols].astype(F32)
        outgoing[:, :, cols] = (
            jnp.dot(spread, value.astype(BF16), preferred_element_type=F32)
            .astype(BF16)
            .reshape(n_ep, PAD, cw)
        )
        returned[pl.ds(e, 1), :, cols] = outgoing[pl.ds(e, 1), :, cols]
        each(lambda d: give_back(d, k).start())
        for i in range(done + k * extra, min(done + (k + 1) * extra, tiles // 2)):
            piece(i)

    for g in range(seg // q_width):
        att_ref[:, g * q_width : (g + 1) * q_width] = (
            acc[g, 0:hd, :] / acc[g, hd : hd + 1, :]
        ).astype(BF16)

    wait_bytes(half_bytes(n_ep - 1), kv_send.at[0])
    wait_bytes(half_bytes(n_ep - 1), kvp_send.at[0])
    wait_bytes(blocks.at[0], pair_send.at[0])
    wait_bytes(blocks.at[0], part_send.at[0])
    wait_bytes(blocks.at[0, pl.ds(0, last)], gath_send.at[0])
    wait_bytes(blocks.at[0, pl.ds(0, last)], red_send.at[0])

    lane_s = lax.broadcasted_iota(jnp.int32, (tokens, slots), 1).astype(F32)
    ones = [jnp.where(lane_s == col, 1.0, 0.0).astype(BF16) for col in slot_cols]
    shares = [own_t[0:tokens, top_count + k : top_count + k + 1] for k in range(top_count)]
    mean = jnp.zeros((tokens, 1), F32)
    for k in range(NCHUNK):
        cols = pl.ds(k * cw, cw)
        wait_bytes(chunk_bytes(returned, k), ret_recv.at[k])
        back = returned[:, :, cols].reshape(slots, cw)
        both = None
        for one, share in zip(ones, shares):
            term = share * jnp.dot(one, back, preferred_element_type=F32)
            both = term if both is None else both + term
        part = residual_scale * x_ref[:, cols].astype(F32) + both
        mixed[:, cols] = part
        mean += jnp.sum(part, axis=-1, keepdims=True)
    centered = mixed[...] - mean / width
    variance = jnp.mean(centered * centered, axis=-1, keepdims=True)
    out_ref[...] = (centered * lax.rsqrt(variance + norm_epsilon) * gain_ref[...]).astype(BF16)
    wait_bytes(outgoing.at[pl.ds(0, n_ep - 1)], ret_send.at[0])


def layer(ids, route, x, gain, qt, q_gain, k_gain, keys, values, gate_t, up_t, down,
          n_ep, n_z, cap, group):
    tokens, width = x.shape
    hidden = down.shape[0]
    head_size, seg = qt.shape
    rows = n_ep * cap
    vmem = pl.BlockSpec(memory_space=pltpu.VMEM)
    hbm = pl.BlockSpec(memory_space=pl.ANY)
    dma = pltpu.SemaphoreType.DMA
    hops = (n_z - 1) * NCHUNK
    groups = seg // Q_WIDTH
    return pl.pallas_call(
        functools.partial(layer_kernel, n_ep, n_z, group),
        out_shape=(
            jax.ShapeDtypeStruct((head_size, seg), BF16),
            jax.ShapeDtypeStruct((tokens, width), BF16),
        ),
        in_specs=[vmem] * 7 + [hbm] * 5,
        out_specs=(vmem, vmem),
        scratch_shapes=[
            pltpu.VMEM((hidden, width), BF16),
            pltpu.VMEM((hidden, width), BF16),
            pltpu.VMEM((width, hidden), BF16),
            pltpu.VMEM((width, hidden), BF16),
            pltpu.VMEM((hidden, width), BF16),
            pltpu.VMEM((seg, 2 * head_size), BF16),
            pltpu.VMEM((seg, 2 * head_size), BF16),
            pltpu.VMEM((n_ep, seg, 2 * head_size), BF16),
            pltpu.VMEM((head_size + 16, n_ep * seg), BF16),
            pltpu.VMEM((groups, 2 * head_size, Q_WIDTH), BF16),
            pltpu.VMEM((K_BLOCK, Q_WIDTH), F32),
            pltpu.VMEM((K_BLOCK, Q_WIDTH), F32),
            pltpu.VMEM((1, Q_WIDTH), F32),
            pltpu.VMEM((groups, 1, Q_WIDTH), F32),
            pltpu.VMEM((groups, head_size + 16, Q_WIDTH), F32),
            pltpu.VMEM((n_ep, PAD, width), BF16),
            pltpu.VMEM((n_ep, PAD, width), BF16),
            pltpu.VMEM((2, n_z, rows, width), BF16),
            pltpu.VMEM((2, n_z, rows, width), BF16),
            pltpu.VMEM((n_z, rows, width), BF16),
            pltpu.VMEM((n_z - 1, rows, width), BF16),
            pltpu.VMEM((n_ep, PAD, width), BF16),
            pltpu.VMEM((tokens, width), F32),
            pltpu.VMEM((8, ids.shape[1]), F32),
            dma((5,)),
            dma((1,)),
            dma((NCHUNK,)),
            dma((1,)),
            dma((hops,)),
            dma((1,)),
            dma((n_z,)),
            dma((1,)),
            dma((n_z,)),
            dma((1,)),
            dma((hops,)),
            dma((1,)),
            dma((NCHUNK,)),
            dma((1,)),
            dma(((n_ep - 1) // KV_GROUP,)),
            dma((1,)),
            dma((1,)),
        ],
        compiler_params=pltpu.CompilerParams(
            collective_id=0, has_side_effects=True, vmem_limit_bytes=VMEM_LIMIT
        ),
    )(ids, route, x, gain, qt, q_gain, k_gain, keys, values, gate_t, up_t, down)


def shards(
    queries,
    keys,
    values,
    query_gain,
    key_gain,
    moe_input,
    expert_ids,
    route_weight,
    gate_weight,
    up_weight,
    down_weight,
    output_gain,
):
    tok_rows = moe_input.shape[0]
    top_count = expert_ids.shape[1]
    n_ep = lax.axis_size("ep")
    n_tp = lax.axis_size("tp")
    cap = max(2, tok_rows * top_count * 5 // (4 * n_ep))
    attended, moe_output = layer(
        expert_ids.T,
        route_weight.T,
        moe_input,
        output_gain[None, :],
        queries.T,
        query_gain[None, :],
        key_gain[None, :],
        keys,
        values,
        gate_weight[0].T,
        up_weight[0].T,
        down_weight[0],
        n_ep,
        n_tp // 2,
        cap,
        QH // KV,
    )
    return (attended.T, moe_output)


def solution(mesh):
    return jax.shard_map(
        shards,
        mesh=mesh,
        in_specs=(
            P("ep", "tp"),
            P("ep", None),
            P("ep", None),
            P(),
            P(),
            P(("ep", "tp"), None),
            P("ep", None),
            P("ep", None),
            P("ep", None, "tp"),
            P("ep", None, "tp"),
            P("ep", "tp", None),
            P(),
        ),
        out_specs=(P("ep", "tp"), P(("ep", "tp"), None)),
        check_vma=False,
    )
```

```python
import functools
import math

import jax
import jax.numpy as jnp
import numpy as np
from jax import lax
from jax.experimental import pallas as pl
from jax.experimental.pallas import tpu as pltpu
from jax.sharding import PartitionSpec as P

QH = 16
KV = 4
GRID_W = 64
MESH = pl.DeviceIdType.MESH
BF16 = jnp.bfloat16
F32 = jnp.float32

rope_theta = 10000.0
rms_epsilon = 1e-06
norm_epsilon = 1e-05
residual_scale = 1.4142135623730951

PAD = 8
NCHUNK = 4
Q_WIDTH = 512
K_BLOCK = 512
PIECES = (0, 2, 3, 5, 6)
LANES = 128
VMEM_LIMIT = 56 * 1024 * 1024
KV_GROUP = 3
KV_FROM = 4


def rotated(heads_t, gain_col, cosines, sines):
    squares = jnp.mean(heads_t * heads_t, axis=0, keepdims=True)
    unit = heads_t * lax.rsqrt(squares + rms_epsilon) * gain_col
    half = heads_t.shape[0] // 2
    a, b = unit[0:half], unit[half:]
    return jnp.concatenate([a * cosines - b * sines, b * cosines + a * sines], axis=0)


def layer_kernel(
    n_ep,
    n_z,
    group,
    ids_hbm,
    route_hbm,
    x_hbm,
    gain_hbm,
    qt_hbm,
    q_gain_hbm,
    k_gain_hbm,
    keys_hbm,
    values_hbm,
    gate_hbm,
    up_hbm,
    down_hbm,
    att_ref,
    out_ref,
    ids_ref,
    route_ref,
    x_ref,
    gain_ref,
    qt_ref,
    q_gain,
    k_gain,
    gate_t,
    up_t,
    gate,
    up,
    down,
    key_cols,
    value_cols,
    kv,
    vt,
    qt,
    s0,
    s1,
    top,
    peak,
    acc,
    outgoing,
    dispatched,
    blocks,
    parts,
    partner_parts,
    ring_in,
    returned,
    mixed,
    meta,
    load_sem,
    disp_send,
    disp_recv,
    gath_send,
    gath_recv,
    pair_send,
    pair_recv,
    part_send,
    part_recv,
    red_send,
    red_recv,
    ret_send,
    ret_recv,
    kv_send,
    kv_recv,
    kvp_send,
    kvp_recv,
):
    e = lax.axis_index("ep")
    t = lax.axis_index("tp")
    z = t // 2
    c = t % 2
    way = 1 - 2 * c
    tokens, width = x_ref.shape
    rows = blocks.shape[2]
    cap = rows // n_ep
    slots = n_ep * PAD
    cw = width // NCHUNK
    last = n_z - 1

    def at_z(distance):
        return lax.rem(z + distance + 2 * n_z, n_z)

    ring_to = (e, at_z(way) * 2 + c)
    partner = (e, z * 2 + 1 - c)

    barrier = pltpu.get_barrier_semaphore()
    for d in range(1, n_ep):
        pl.semaphore_signal(
            barrier, inc=1, device_id=(lax.rem(e + d, n_ep), t), device_id_type=MESH
        )
    for peer in ((e, at_z(1) * 2 + c), (e, at_z(-1) * 2 + c), partner):
        pl.semaphore_signal(barrier, inc=1, device_id=peer, device_id_type=MESH)

    hd = q_gain.shape[1]
    seg = qt_ref.shape[1]
    key_head = t // group
    head_cols = pl.ds(pl.multiple_of(key_head // 2 * (2 * hd), 2 * hd), 2 * hd)
    loads = [
        pltpu.make_async_copy(src, dst, load_sem.at[i])
        for i, (src, dst) in enumerate(
            (
                (ids_hbm, ids_ref),
                (route_hbm, route_ref),
                (x_hbm, x_ref),
                (k_gain_hbm, k_gain),
                (keys_hbm.at[:, head_cols], key_cols),
                (values_hbm.at[:, head_cols], value_cols),
                (gate_hbm, gate_t),
                (up_hbm, up_t),
                (q_gain_hbm, q_gain),
                (qt_hbm, qt_ref),
                (down_hbm, down),
                (gain_hbm, gain_ref),
            )
        )
    ]
    for load in loads:
        load.start()

    top_count = ids_ref.shape[0]
    column_tokens = ids_ref.shape[1]
    for load in loads[0:3]:
        load.wait()
    meta[...] = jnp.zeros(meta.shape, F32)
    meta[0:top_count, :] = ids_ref[...].astype(F32)
    meta[top_count : 2 * top_count, :] = route_ref[...]
    own = pltpu.roll(
        meta[...], lax.rem(column_tokens - t * tokens, column_tokens), axis=1
    )[:, 0:LANES]
    own_t = own.T
    sub_i = lax.broadcasted_iota(jnp.int32, (LANES, LANES), 0)
    lane_i = lax.broadcasted_iota(jnp.int32, (LANES, LANES), 1)
    slot_rows, slot_cols = [], []
    for k in range(top_count):
        row, col = own[k : k + 1, :], own_t[:, k : k + 1]
        hit_r = sum(jnp.where(own_t[:, j : j + 1] == row, 1.0, 0.0) for j in range(top_count))
        hit_c = sum(jnp.where(own[j : j + 1, :] == col, 1.0, 0.0) for j in range(top_count))
        rank_r = jnp.sum(jnp.where(sub_i < lane_i, hit_r, 0.0), axis=0, keepdims=True)
        rank_c = jnp.sum(jnp.where(lane_i < sub_i, hit_c, 0.0), axis=1, keepdims=True)
        slot_rows.append((row * PAD + rank_r)[:, 0:tokens])
        slot_cols.append((col * PAD + rank_c)[0:tokens, :])

    slot = lax.broadcasted_iota(jnp.int32, (slots, tokens), 0).astype(F32)
    pick = sum(jnp.where(slot == row, 1.0, 0.0) for row in slot_rows)
    outgoing[...] = (
        jnp.dot(pick.astype(BF16), x_ref[...], preferred_element_type=F32)
        .astype(BF16)
        .reshape(n_ep, PAD, width)
    )
    dispatched[pl.ds(e, 1)] = outgoing[pl.ds(e, 1)]
    pl.semaphore_wait(barrier, n_ep - 1 + 3)

    def exchange(src, dst, send, recv, d, k):
        to = lax.rem(e + d, n_ep)
        cols = pl.ds(k * cw, cw)
        return pltpu.make_async_remote_copy(
            src_ref=src.at[to, :, cols],
            dst_ref=dst.at[e, :, cols],
            send_sem=send.at[0],
            recv_sem=recv.at[k],
            device_id=(to, t),
            device_id_type=MESH,
        )

    def each(act):
        def one(d, carry):
            act(d)
            return carry

        lax.fori_loop(1, n_ep, one, 0)

    def dispatch(d, k):
        return exchange(outgoing, dispatched, disp_send, disp_recv, d, k)

    def give_back(d, k):
        return exchange(outgoing, returned, ret_send, ret_recv, d, k)

    def wait_bytes(ref, sem):
        pltpu.make_async_copy(ref, ref, sem).wait()

    def chunk_bytes(ref, k):
        return ref.at[pl.ds(0, n_ep - 1), :, pl.ds(k * cw, cw)]

    for k in range(NCHUNK):
        each(lambda d: dispatch(d, k).start())
    def kv_copy(d):
        rows_c = pl.ds(pl.multiple_of(c * (seg // 2), seg // 2), seg // 2)
        return pltpu.make_async_remote_copy(
            src_ref=kv.at[e, rows_c, :],
            dst_ref=kv.at[e, rows_c, :],
            send_sem=kv_send.at[0],
            recv_sem=kv_recv.at[(d - 1) // KV_GROUP],
            device_id=(lax.rem(e + d, n_ep), t),
            device_id_type=MESH,
        )

    def kv_pair_copy(d):
        rows_c = pl.ds(pl.multiple_of(c * (seg // 2), seg // 2), seg // 2)
        ref = kv.at[lax.rem(e - d + n_ep, n_ep), rows_c, :]
        return pltpu.make_async_remote_copy(
            src_ref=ref,
            dst_ref=ref,
            send_sem=kvp_send.at[0],
            recv_sem=kvp_recv.at[0],
            device_id=partner,
            device_id_type=MESH,
        )

    lane = lax.broadcasted_iota(jnp.int32, (1, seg), 1)
    position = e * seg + lane
    grid_row = (position // GRID_W).astype(F32)
    grid_col = (position % GRID_W).astype(F32)
    quarter = hd // 4
    freq_i = lax.broadcasted_iota(jnp.int32, (quarter, 1), 0)
    inverse = jnp.zeros((quarter, 1), F32)
    for j in range(quarter):
        inverse = jnp.where(freq_i == j, float(np.float32(rope_theta ** (-j / quarter))), inverse)
    angles = jnp.concatenate([inverse * grid_row, inverse * grid_col], axis=0)
    gain_eye = lax.broadcasted_iota(jnp.int32, (hd, hd), 0) == lax.broadcasted_iota(
        jnp.int32, (hd, hd), 1
    )

    def column(row_ref):
        return jnp.sum(jnp.where(gain_eye, row_ref[...], 0.0), axis=1, keepdims=True)

    cosines, sines = jnp.cos(angles), jnp.sin(angles)
    odd = key_head % 2 == 1
    for load in loads[3:6]:
        load.wait()
    keys_t = key_cols[...].T.astype(F32)
    values_t = value_cols[...].T.astype(F32)
    own_k = rotated(jnp.where(odd, keys_t[hd:], keys_t[:hd]), column(k_gain), cosines, sines)
    own_v = jnp.where(odd, values_t[hd:], values_t[:hd])
    kv[pl.ds(e, 1)] = (
        jnp.concatenate([own_k.astype(BF16), own_v.astype(BF16)], axis=0)
        .T.reshape(1, seg, 2 * hd)
    )
    for load in loads[6:8]:
        load.wait()
    step = width // NCHUNK
    for k in range(NCHUNK):
        gate[k * step : (k + 1) * step, :] = gate_t[:, k * step : (k + 1) * step].T
        up[k * step : (k + 1) * step, :] = up_t[:, k * step : (k + 1) * step].T

    def gather_copy(s, k):
        ref = blocks.at[c, at_z(-way * s), :, pl.ds(k * cw, cw)]
        return pltpu.make_async_remote_copy(
            src_ref=ref,
            dst_ref=ref,
            send_sem=gath_send.at[0],
            recv_sem=gath_recv.at[s * NCHUNK + k],
            device_id=ring_to,
            device_id_type=MESH,
        )

    def pair_copy(s):
        ref = blocks.at[c, at_z(-way * s)]
        return pltpu.make_async_remote_copy(
            src_ref=ref,
            dst_ref=ref,
            send_sem=pair_send.at[0],
            recv_sem=pair_recv.at[s],
            device_id=partner,
            device_id_type=MESH,
        )

    def part_copy(s):
        return pltpu.make_async_remote_copy(
            src_ref=parts.at[1 - c, at_z(way * s)],
            dst_ref=partner_parts.at[at_z(way * s)],
            send_sem=part_send.at[0],
            recv_sem=part_recv.at[s],
            device_id=partner,
            device_id_type=MESH,
        )

    def reduce_copy(s, k):
        cols = pl.ds(k * cw, cw)
        return pltpu.make_async_remote_copy(
            src_ref=parts.at[c, at_z(-way * (s + 1)), :, cols],
            dst_ref=ring_in.at[s, :, cols],
            send_sem=red_send.at[0],
            recv_sem=red_recv.at[s * NCHUNK + k],
            device_id=ring_to,
            device_id_type=MESH,
        )

    def feed(ring, zi):
        xb = blocks[pl.ds(ring, 1), pl.ds(zi, 1)].reshape(rows, width)
        g = jnp.dot(xb, gate[...], preferred_element_type=F32)
        u = jnp.dot(xb, up[...], preferred_element_type=F32)
        hidden = ((g / (1.0 + jnp.exp(-g))) * u).astype(BF16)
        part = jnp.dot(hidden, down[...], preferred_element_type=F32).astype(BF16)
        parts[pl.ds(ring, 1), pl.ds(zi, 1)] = part.reshape(1, 1, rows, width)

    def feed_own(s):
        feed(c, at_z(-way * s))

    def feed_partner(s):
        pair_copy(s).wait_recv()
        feed(1 - c, at_z(way * s))
        part_copy(s).start()

    kb = s0.shape[0]
    q_width = s0.shape[1]
    nk = n_ep * seg // kb
    tiles = nk * (seg // q_width)
    score_scale = hd**-0.5 * math.log2(math.e)

    def score(n, sref):
        rows_n = pl.ds(pl.multiple_of(lax.rem(n, nk) * kb, kb), kb)
        flat = kv.reshape(n_ep * seg, 2 * hd)
        q = qt[pl.ds(n // nk, 1)].reshape(2 * hd, q_width)
        sc = jnp.dot(flat[rows_n, :], q, preferred_element_type=F32)
        sref[...] = sc
        return jnp.max(sc, axis=0, keepdims=True)

    def absorb(n, sref, state, best):
        m, total = state
        cols_n = pl.ds(pl.multiple_of(lax.rem(n, nk) * kb, kb), kb)
        new = jnp.maximum(m, best)
        p = jnp.exp2((sref[...] - new) * score_scale).astype(BF16)
        shrink = jnp.exp2((m - new) * score_scale)
        return new, total * shrink + jnp.dot(vt[:, cols_n], p, preferred_element_type=F32)

    def piece(i):
        n = 2 * i
        group_i = pl.ds(n // nk, 1)
        best0 = top[...]
        state = (peak[group_i].reshape(1, q_width), acc[group_i].reshape(hd + 16, q_width))
        best1 = score(n + 1, s1)
        state = absorb(n, s0, state, best0)
        best2 = score(jnp.minimum(n + 2, tiles - 1), s0)
        m, total = absorb(n + 1, s1, state, best1)
        top[...] = best2
        peak[group_i] = m.reshape(1, 1, q_width)
        acc[group_i] = total.reshape(1, hd + 16, q_width)

    r_i = lax.broadcasted_iota(jnp.int32, (rows, slots), 0)
    s_i = lax.broadcasted_iota(jnp.int32, (rows, slots), 1)
    squeeze = jnp.where(s_i == (r_i // cap) * PAD + r_i % cap, 1.0, 0.0).astype(BF16)
    for k in range(NCHUNK):
        cols = pl.ds(k * cw, cw)
        wait_bytes(chunk_bytes(dispatched, k), disp_recv.at[k])
        came = dispatched[:, :, cols].reshape(slots, cw)
        blocks[pl.ds(c, 1), pl.ds(z, 1), :, cols] = (
            jnp.dot(squeeze, came, preferred_element_type=F32)
            .astype(BF16)
            .reshape(1, 1, rows, cw)
        )
        gather_copy(0, k).start()
    pair_copy(0).start()
    each(lambda d: kv_copy(d).start())
    for load in loads[8:]:
        load.wait()
    own_q = rotated(qt_ref[...].astype(F32), column(q_gain), cosines, sines).astype(BF16)
    for g in range(seg // q_width):
        qt[g, 0:hd, :] = own_q[:, g * q_width : (g + 1) * q_width]
        qt[g, hd : 2 * hd, :] = jnp.zeros((hd, q_width), BF16)
    peak[...] = jnp.full(peak.shape, -jnp.inf, F32)
    acc[...] = jnp.zeros(acc.shape, F32)

    def half_bytes(n):
        return kv.at[pl.ds(0, n), pl.ds(0, seg // 2), :]

    def kv_forward(g):
        wait_bytes(half_bytes(KV_GROUP), kv_recv.at[g])
        for i in range(KV_GROUP):
            kv_pair_copy(g * KV_GROUP + 1 + i).start()

    def gather_step(s, carry):
        def forward(k):
            gather_copy(s, k).wait_recv()
            gather_copy(s + 1, k).start()

        forward(0)
        forward(1)
        feed_own(s)
        forward(2)

        @pl.when(s >= KV_FROM)
        def _():
            kv_forward(s - KV_FROM)

        feed_partner(s)
        forward(3)
        pair_copy(s + 1).start()
        return carry

    lax.fori_loop(0, last - 1, gather_step, 0)

    def first_hop(k):
        b = at_z(-way)
        cols = pl.ds(k * cw, cw)
        value = parts[pl.ds(c, 1), pl.ds(b, 1), :, cols].astype(F32).reshape(rows, cw)
        value += partner_parts[pl.ds(b, 1), :, cols].astype(F32).reshape(rows, cw)
        parts[pl.ds(c, 1), pl.ds(b, 1), :, cols] = value.astype(BF16).reshape(1, 1, rows, cw)
        reduce_copy(0, k).start()

    part_copy(1).wait_recv()
    for k in range(NCHUNK):
        first_hop(k)
    for g in range(last - 1 - KV_FROM, (n_ep - 1) // KV_GROUP):
        kv_forward(g)
    feed_own(last - 1)
    feed_partner(last - 1)
    for k in range(NCHUNK):
        gather_copy(last - 1, k).wait_recv()
    pair_copy(last).start()
    feed_own(last)
    feed_partner(last)

    def turn(j, carry):
        cols = pl.ds(pl.multiple_of(j * seg, seg), seg)
        vt[0:hd, cols] = kv[pl.ds(j, 1)].reshape(seg, 2 * hd).T[hd : 2 * hd]
        vt[hd : hd + 16, cols] = jnp.ones((16, seg), BF16)
        return carry

    def reduce_step(s, carry):
        b = at_z(-way * (s + 1))
        part_copy(s + 1).wait_recv()
        for k in range(NCHUNK):
            cols = pl.ds(k * cw, cw)
            value = parts[pl.ds(c, 1), pl.ds(b, 1), :, cols].astype(F32).reshape(rows, cw)
            value += partner_parts[pl.ds(b, 1), :, cols].astype(F32).reshape(rows, cw)
            reduce_copy(s - 1, k).wait_recv()
            value += ring_in[pl.ds(s - 1, 1), :, cols].astype(F32).reshape(rows, cw)
            parts[pl.ds(c, 1), pl.ds(b, 1), :, cols] = value.astype(BF16).reshape(1, 1, rows, cw)
            reduce_copy(s, k).start()

            @pl.when(s > 1)
            def _():
                for i in range(PIECES[k], PIECES[k + 1]):
                    piece((s - 2) * PIECES[-1] + i)

        @pl.when(s == 1)
        def _():
            wait_bytes(half_bytes(n_ep - 1), kvp_recv.at[0])
            lax.fori_loop(0, n_ep, turn, 0)
            top[...] = score(0, s0)

        return carry

    lax.fori_loop(1, last, reduce_step, 0)

    r_j = lax.broadcasted_iota(jnp.int32, (slots, rows), 1)
    s_j = lax.broadcasted_iota(jnp.int32, (slots, rows), 0)
    spread = jnp.where(s_j == (r_j // cap) * PAD + r_j % cap, 1.0, 0.0).astype(BF16)
    wait_bytes(outgoing.at[pl.ds(0, n_ep - 1)], disp_send.at[0])
    part_copy(0).wait_recv()
    done = (last - 2) * PIECES[-1]
    extra = -(-(tiles // 2 - done) // NCHUNK)
    for k in range(NCHUNK):
        cols = pl.ds(k * cw, cw)
        value = parts[pl.ds(c, 1), pl.ds(z, 1), :, cols].astype(F32).reshape(rows, cw)
        value += partner_parts[pl.ds(z, 1), :, cols].astype(F32).reshape(rows, cw)
        reduce_copy(last - 1, k).wait_recv()
        value += ring_in[last - 1, :, cols].astype(F32)
        outgoing[:, :, cols] = (
            jnp.dot(spread, value.astype(BF16), preferred_element_type=F32)
            .astype(BF16)
            .reshape(n_ep, PAD, cw)
        )
        returned[pl.ds(e, 1), :, cols] = outgoing[pl.ds(e, 1), :, cols]
        each(lambda d: give_back(d, k).start())
        for i in range(done + k * extra, min(done + (k + 1) * extra, tiles // 2)):
            piece(i)

    for g in range(seg // q_width):
        att_ref[:, g * q_width : (g + 1) * q_width] = (
            acc[g, 0:hd, :] / acc[g, hd : hd + 1, :]
        ).astype(BF16)

    wait_bytes(half_bytes(n_ep - 1), kv_send.at[0])
    wait_bytes(half_bytes(n_ep - 1), kvp_send.at[0])
    wait_bytes(blocks.at[0], pair_send.at[0])
    wait_bytes(blocks.at[0], part_send.at[0])
    wait_bytes(blocks.at[0, pl.ds(0, last)], gath_send.at[0])
    wait_bytes(blocks.at[0, pl.ds(0, last)], red_send.at[0])

    lane_s = lax.broadcasted_iota(jnp.int32, (tokens, slots), 1).astype(F32)
    ones = [jnp.where(lane_s == col, 1.0, 0.0).astype(BF16) for col in slot_cols]
    shares = [own_t[0:tokens, top_count + k : top_count + k + 1] for k in range(top_count)]
    mean = jnp.zeros((tokens, 1), F32)
    for k in range(NCHUNK):
        cols = pl.ds(k * cw, cw)
        wait_bytes(chunk_bytes(returned, k), ret_recv.at[k])
        back = returned[:, :, cols].reshape(slots, cw)
        both = None
        for one, share in zip(ones, shares):
            term = share * jnp.dot(one, back, preferred_element_type=F32)
            both = term if both is None else both + term
        part = residual_scale * x_ref[:, cols].astype(F32) + both
        mixed[:, cols] = part
        mean += jnp.sum(part, axis=-1, keepdims=True)
    centered = mixed[...] - mean / width
    variance = jnp.mean(centered * centered, axis=-1, keepdims=True)
    out_ref[...] = (centered * lax.rsqrt(variance + norm_epsilon) * gain_ref[...]).astype(BF16)
    wait_bytes(outgoing.at[pl.ds(0, n_ep - 1)], ret_send.at[0])


def layer(ids, route, x, gain, qt, q_gain, k_gain, keys, values, gate_t, up_t, down,
          n_ep, n_z, cap, group):
    tokens, width = x.shape
    hidden = down.shape[0]
    head_size, seg = qt.shape
    rows = n_ep * cap
    vmem = pl.BlockSpec(memory_space=pltpu.VMEM)
    hbm = pl.BlockSpec(memory_space=pltpu.HBM)
    dma = pltpu.SemaphoreType.DMA
    hops = (n_z - 1) * NCHUNK
    groups = seg // Q_WIDTH
    return pl.pallas_call(
        functools.partial(layer_kernel, n_ep, n_z, group),
        out_shape=(
            pltpu.VMEM((head_size, seg), BF16),
            pltpu.VMEM((tokens, width), BF16),
        ),
        in_specs=[hbm] * 12,
        out_specs=(vmem, vmem),
        scratch_shapes=[
            pltpu.VMEM(ids.shape, ids.dtype),
            pltpu.VMEM(route.shape, F32),
            pltpu.VMEM((tokens, width), BF16),
            pltpu.VMEM((1, width), F32),
            pltpu.VMEM((head_size, seg), BF16),
            pltpu.VMEM((1, head_size), F32),
            pltpu.VMEM((1, head_size), F32),
            pltpu.VMEM((hidden, width), BF16),
            pltpu.VMEM((hidden, width), BF16),
            pltpu.VMEM((width, hidden), BF16),
            pltpu.VMEM((width, hidden), BF16),
            pltpu.VMEM((hidden, width), BF16),
            pltpu.VMEM((seg, 2 * head_size), BF16),
            pltpu.VMEM((seg, 2 * head_size), BF16),
            pltpu.VMEM((n_ep, seg, 2 * head_size), BF16),
            pltpu.VMEM((head_size + 16, n_ep * seg), BF16),
            pltpu.VMEM((groups, 2 * head_size, Q_WIDTH), BF16),
            pltpu.VMEM((K_BLOCK, Q_WIDTH), F32),
            pltpu.VMEM((K_BLOCK, Q_WIDTH), F32),
            pltpu.VMEM((1, Q_WIDTH), F32),
            pltpu.VMEM((groups, 1, Q_WIDTH), F32),
            pltpu.VMEM((groups, head_size + 16, Q_WIDTH), F32),
            pltpu.VMEM((n_ep, PAD, width), BF16),
            pltpu.VMEM((n_ep, PAD, width), BF16),
            pltpu.VMEM((2, n_z, rows, width), BF16),
            pltpu.VMEM((2, n_z, rows, width), BF16),
            pltpu.VMEM((n_z, rows, width), BF16),
            pltpu.VMEM((n_z - 1, rows, width), BF16),
            pltpu.VMEM((n_ep, PAD, width), BF16),
            pltpu.VMEM((tokens, width), F32),
            pltpu.VMEM((8, ids.shape[1]), F32),
            dma((12,)),
            dma((1,)),
            dma((NCHUNK,)),
            dma((1,)),
            dma((hops,)),
            dma((1,)),
            dma((n_z,)),
            dma((1,)),
            dma((n_z,)),
            dma((1,)),
            dma((hops,)),
            dma((1,)),
            dma((NCHUNK,)),
            dma((1,)),
            dma(((n_ep - 1) // KV_GROUP,)),
            dma((1,)),
            dma((1,)),
        ],
        compiler_params=pltpu.CompilerParams(
            collective_id=0, has_side_effects=True, vmem_limit_bytes=VMEM_LIMIT
        ),
    )(ids, route, x, gain, qt, q_gain, k_gain, keys, values, gate_t, up_t, down)


def shards(
    queries,
    keys,
    values,
    query_gain,
    key_gain,
    moe_input,
    expert_ids,
    route_weight,
    gate_weight,
    up_weight,
    down_weight,
    output_gain,
):
    tok_rows = moe_input.shape[0]
    top_count = expert_ids.shape[1]
    n_ep = lax.axis_size("ep")
    n_tp = lax.axis_size("tp")
    cap = max(2, tok_rows * top_count * 5 // (4 * n_ep))
    attended, moe_output = layer(
        expert_ids.T,
        route_weight.T,
        moe_input,
        output_gain[None, :],
        queries.T,
        query_gain[None, :],
        key_gain[None, :],
        keys,
        values,
        gate_weight[0].T,
        up_weight[0].T,
        down_weight[0],
        n_ep,
        n_tp // 2,
        cap,
        QH // KV,
    )
    return (attended.T, moe_output)


def solution(mesh):
    return jax.shard_map(
        shards,
        mesh=mesh,
        in_specs=(
            P("ep", "tp"),
            P("ep", None),
            P("ep", None),
            P(),
            P(),
            P(("ep", "tp"), None),
            P("ep", None),
            P("ep", None),
            P("ep", None, "tp"),
            P("ep", None, "tp"),
            P("ep", "tp", None),
            P(),
        ),
        out_specs=(P("ep", "tp"), P(("ep", "tp"), None)),
        check_vma=False,
    )
```

```python
import functools
import math

import jax
import jax.numpy as jnp
import numpy as np
from jax import lax
from jax.experimental import pallas as pl
from jax.experimental.pallas import tpu as pltpu
from jax.sharding import PartitionSpec as P

QH = 16
KV = 4
GRID_W = 64
MESH = pl.DeviceIdType.MESH
BF16 = jnp.bfloat16
F32 = jnp.float32

rope_theta = 10000.0
rms_epsilon = 1e-06
norm_epsilon = 1e-05
residual_scale = 1.4142135623730951

PAD = 8
NCHUNK = 4
Q_WIDTH = 512
K_BLOCK = 512
PIECES = (0, 2, 3, 5, 6)
LANES = 128
VMEM_LIMIT = 56 * 1024 * 1024
KV_GROUP = 3
KV_FROM = 4


def rotated(heads_t, gain_col, cosines, sines):
    squares = jnp.mean(heads_t * heads_t, axis=0, keepdims=True)
    unit = heads_t * lax.rsqrt(squares + rms_epsilon) * gain_col
    half = heads_t.shape[0] // 2
    a, b = unit[0:half], unit[half:]
    return jnp.concatenate([a * cosines - b * sines, b * cosines + a * sines], axis=0)


def layer_kernel(
    n_ep,
    n_z,
    group,
    ids_hbm,
    route_hbm,
    x_hbm,
    gain_hbm,
    qt_hbm,
    q_gain_hbm,
    k_gain_hbm,
    keys_hbm,
    values_hbm,
    gate_hbm,
    up_hbm,
    down_hbm,
    att_ref,
    out_ref,
    ids_ref,
    route_ref,
    x_ref,
    gain_ref,
    qt_ref,
    q_gain,
    k_gain,
    gate_t,
    up_t,
    gate,
    up,
    down,
    key_cols,
    value_cols,
    kv,
    vt,
    qt,
    s0,
    s1,
    top,
    peak,
    acc,
    outgoing,
    dispatched,
    blocks,
    parts,
    partner_parts,
    ring_in,
    returned,
    mixed,
    meta,
    load_sem,
    disp_send,
    disp_recv,
    gath_send,
    gath_recv,
    pair_send,
    pair_recv,
    part_send,
    part_recv,
    red_send,
    red_recv,
    ret_send,
    ret_recv,
    kv_send,
    kv_recv,
    kvp_send,
    kvp_recv,
):
    e = lax.axis_index("ep")
    t = lax.axis_index("tp")
    z = t // 2
    c = t % 2
    way = 1 - 2 * c
    tokens, width = x_ref.shape
    rows = blocks.shape[2]
    cap = rows // n_ep
    slots = n_ep * PAD
    cw = width // NCHUNK
    last = n_z - 1

    def at_z(distance):
        return lax.rem(z + distance + 2 * n_z, n_z)

    ring_to = (e, at_z(way) * 2 + c)
    partner = (e, z * 2 + 1 - c)

    hd = q_gain.shape[1]
    seg = qt_ref.shape[1]
    key_head = t // group
    head_cols = pl.ds(pl.multiple_of(key_head // 2 * (2 * hd), 2 * hd), 2 * hd)
    loads = [
        pltpu.make_async_copy(src, dst, load_sem.at[i])
        for i, (src, dst) in enumerate(
            (
                (ids_hbm, ids_ref),
                (route_hbm, route_ref),
                (x_hbm, x_ref),
                (k_gain_hbm, k_gain),
                (keys_hbm.at[:, head_cols], key_cols),
                (values_hbm.at[:, head_cols], value_cols),
                (gate_hbm, gate_t),
                (up_hbm, up_t),
                (q_gain_hbm, q_gain),
                (qt_hbm, qt_ref),
                (down_hbm, down),
                (gain_hbm, gain_ref),
            )
        )
    ]
    for load in loads:
        load.start()

    barrier = pltpu.get_barrier_semaphore()
    for d in range(1, n_ep):
        pl.semaphore_signal(
            barrier, inc=1, device_id=(lax.rem(e + d, n_ep), t), device_id_type=MESH
        )
    for peer in ((e, at_z(1) * 2 + c), (e, at_z(-1) * 2 + c), partner):
        pl.semaphore_signal(barrier, inc=1, device_id=peer, device_id_type=MESH)

    top_count = ids_ref.shape[0]
    column_tokens = ids_ref.shape[1]
    for load in loads[0:3]:
        load.wait()
    meta[...] = jnp.zeros(meta.shape, F32)
    meta[0:top_count, :] = ids_ref[...].astype(F32)
    meta[top_count : 2 * top_count, :] = route_ref[...]
    own = pltpu.roll(
        meta[...], lax.rem(column_tokens - t * tokens, column_tokens), axis=1
    )[:, 0:LANES]
    own_t = own.T
    sub_i = lax.broadcasted_iota(jnp.int32, (LANES, LANES), 0)
    lane_i = lax.broadcasted_iota(jnp.int32, (LANES, LANES), 1)
    slot_rows, slot_cols = [], []
    for k in range(top_count):
        row, col = own[k : k + 1, :], own_t[:, k : k + 1]
        hit_r = sum(jnp.where(own_t[:, j : j + 1] == row, 1.0, 0.0) for j in range(top_count))
        hit_c = sum(jnp.where(own[j : j + 1, :] == col, 1.0, 0.0) for j in range(top_count))
        rank_r = jnp.sum(jnp.where(sub_i < lane_i, hit_r, 0.0), axis=0, keepdims=True)
        rank_c = jnp.sum(jnp.where(lane_i < sub_i, hit_c, 0.0), axis=1, keepdims=True)
        slot_rows.append((row * PAD + rank_r)[:, 0:tokens])
        slot_cols.append((col * PAD + rank_c)[0:tokens, :])

    slot = lax.broadcasted_iota(jnp.int32, (slots, tokens), 0).astype(F32)
    pick = sum(jnp.where(slot == row, 1.0, 0.0) for row in slot_rows)
    pick = pick.astype(BF16)

    def gather_rows(k):
        cols = pl.ds(k * cw, cw)
        outgoing[:, :, cols] = (
            jnp.dot(pick, x_ref[:, cols], preferred_element_type=F32)
            .astype(BF16)
            .reshape(n_ep, PAD, cw)
        )
        dispatched[pl.ds(e, 1), :, cols] = outgoing[pl.ds(e, 1), :, cols]

    gather_rows(0)
    pl.semaphore_wait(barrier, n_ep - 1 + 3)

    def exchange(src, dst, send, recv, d, k):
        to = lax.rem(e + d, n_ep)
        cols = pl.ds(k * cw, cw)
        return pltpu.make_async_remote_copy(
            src_ref=src.at[to, :, cols],
            dst_ref=dst.at[e, :, cols],
            send_sem=send.at[0],
            recv_sem=recv.at[k],
            device_id=(to, t),
            device_id_type=MESH,
        )

    def each(act):
        def one(d, carry):
            act(d)
            return carry

        lax.fori_loop(1, n_ep, one, 0)

    def dispatch(d, k):
        return exchange(outgoing, dispatched, disp_send, disp_recv, d, k)

    def give_back(d, k):
        return exchange(outgoing, returned, ret_send, ret_recv, d, k)

    def wait_bytes(ref, sem):
        pltpu.make_async_copy(ref, ref, sem).wait()

    def chunk_bytes(ref, k):
        return ref.at[pl.ds(0, n_ep - 1), :, pl.ds(k * cw, cw)]

    for k in range(NCHUNK):
        if k:
            gather_rows(k)
        each(lambda d: dispatch(d, k).start())
    def kv_copy(d):
        rows_c = pl.ds(pl.multiple_of(c * (seg // 2), seg // 2), seg // 2)
        return pltpu.make_async_remote_copy(
            src_ref=kv.at[e, rows_c, :],
            dst_ref=kv.at[e, rows_c, :],
            send_sem=kv_send.at[0],
            recv_sem=kv_recv.at[(d - 1) // KV_GROUP],
            device_id=(lax.rem(e + d, n_ep), t),
            device_id_type=MESH,
        )

    def kv_pair_copy(d):
        rows_c = pl.ds(pl.multiple_of(c * (seg // 2), seg // 2), seg // 2)
        ref = kv.at[lax.rem(e - d + n_ep, n_ep), rows_c, :]
        return pltpu.make_async_remote_copy(
            src_ref=ref,
            dst_ref=ref,
            send_sem=kvp_send.at[0],
            recv_sem=kvp_recv.at[0],
            device_id=partner,
            device_id_type=MESH,
        )

    lane = lax.broadcasted_iota(jnp.int32, (1, seg), 1)
    position = e * seg + lane
    grid_row = (position // GRID_W).astype(F32)
    grid_col = (position % GRID_W).astype(F32)
    quarter = hd // 4
    freq_i = lax.broadcasted_iota(jnp.int32, (quarter, 1), 0)
    inverse = jnp.zeros((quarter, 1), F32)
    for j in range(quarter):
        inverse = jnp.where(freq_i == j, float(np.float32(rope_theta ** (-j / quarter))), inverse)
    angles = jnp.concatenate([inverse * grid_row, inverse * grid_col], axis=0)
    gain_eye = lax.broadcasted_iota(jnp.int32, (hd, hd), 0) == lax.broadcasted_iota(
        jnp.int32, (hd, hd), 1
    )

    def column(row_ref):
        return jnp.sum(jnp.where(gain_eye, row_ref[...], 0.0), axis=1, keepdims=True)

    cosines, sines = jnp.cos(angles), jnp.sin(angles)
    odd = key_head % 2 == 1
    for load in loads[3:6]:
        load.wait()
    keys_t = key_cols[...].T.astype(F32)
    values_t = value_cols[...].T.astype(F32)
    own_k = rotated(jnp.where(odd, keys_t[hd:], keys_t[:hd]), column(k_gain), cosines, sines)
    own_v = jnp.where(odd, values_t[hd:], values_t[:hd])
    kv[pl.ds(e, 1)] = (
        jnp.concatenate([own_k.astype(BF16), own_v.astype(BF16)], axis=0)
        .T.reshape(1, seg, 2 * hd)
    )
    for load in loads[6:8]:
        load.wait()
    step = width // NCHUNK
    for k in range(NCHUNK):
        gate[k * step : (k + 1) * step, :] = gate_t[:, k * step : (k + 1) * step].T
        up[k * step : (k + 1) * step, :] = up_t[:, k * step : (k + 1) * step].T

    def gather_copy(s, k):
        ref = blocks.at[c, at_z(-way * s), :, pl.ds(k * cw, cw)]
        return pltpu.make_async_remote_copy(
            src_ref=ref,
            dst_ref=ref,
            send_sem=gath_send.at[0],
            recv_sem=gath_recv.at[s * NCHUNK + k],
            device_id=ring_to,
            device_id_type=MESH,
        )

    def pair_copy(s):
        ref = blocks.at[c, at_z(-way * s)]
        return pltpu.make_async_remote_copy(
            src_ref=ref,
            dst_ref=ref,
            send_sem=pair_send.at[0],
            recv_sem=pair_recv.at[s],
            device_id=partner,
            device_id_type=MESH,
        )

    def part_copy(s):
        return pltpu.make_async_remote_copy(
            src_ref=parts.at[1 - c, at_z(way * s)],
            dst_ref=partner_parts.at[at_z(way * s)],
            send_sem=part_send.at[0],
            recv_sem=part_recv.at[s],
            device_id=partner,
            device_id_type=MESH,
        )

    def reduce_copy(s, k):
        cols = pl.ds(k * cw, cw)
        return pltpu.make_async_remote_copy(
            src_ref=parts.at[c, at_z(-way * (s + 1)), :, cols],
            dst_ref=ring_in.at[s, :, cols],
            send_sem=red_send.at[0],
            recv_sem=red_recv.at[s * NCHUNK + k],
            device_id=ring_to,
            device_id_type=MESH,
        )

    def feed(ring, zi):
        xb = blocks[pl.ds(ring, 1), pl.ds(zi, 1)].reshape(rows, width)
        g = jnp.dot(xb, gate[...], preferred_element_type=F32)
        u = jnp.dot(xb, up[...], preferred_element_type=F32)
        hidden = ((g / (1.0 + jnp.exp(-g))) * u).astype(BF16)
        part = jnp.dot(hidden, down[...], preferred_element_type=F32).astype(BF16)
        parts[pl.ds(ring, 1), pl.ds(zi, 1)] = part.reshape(1, 1, rows, width)

    def feed_own(s):
        feed(c, at_z(-way * s))

    def feed_partner(s):
        pair_copy(s).wait_recv()
        feed(1 - c, at_z(way * s))
        part_copy(s).start()

    kb = s0.shape[0]
    q_width = s0.shape[1]
    nk = n_ep * seg // kb
    tiles = nk * (seg // q_width)
    score_scale = hd**-0.5 * math.log2(math.e)

    def score(n, sref):
        rows_n = pl.ds(pl.multiple_of(lax.rem(n, nk) * kb, kb), kb)
        flat = kv.reshape(n_ep * seg, 2 * hd)
        q = qt[pl.ds(n // nk, 1)].reshape(2 * hd, q_width)
        sc = jnp.dot(flat[rows_n, :], q, preferred_element_type=F32)
        sref[...] = sc
        return jnp.max(sc, axis=0, keepdims=True)

    def absorb(n, sref, state, best):
        m, total = state
        cols_n = pl.ds(pl.multiple_of(lax.rem(n, nk) * kb, kb), kb)
        new = jnp.maximum(m, best)
        p = jnp.exp2((sref[...] - new) * score_scale).astype(BF16)
        shrink = jnp.exp2((m - new) * score_scale)
        return new, total * shrink + jnp.dot(vt[:, cols_n], p, preferred_element_type=F32)

    def piece(i):
        n = 2 * i
        group_i = pl.ds(n // nk, 1)
        best0 = top[...]
        state = (peak[group_i].reshape(1, q_width), acc[group_i].reshape(hd + 16, q_width))
        best1 = score(n + 1, s1)
        state = absorb(n, s0, state, best0)
        best2 = score(jnp.minimum(n + 2, tiles - 1), s0)
        m, total = absorb(n + 1, s1, state, best1)
        top[...] = best2
        peak[group_i] = m.reshape(1, 1, q_width)
        acc[group_i] = total.reshape(1, hd + 16, q_width)

    r_i = lax.broadcasted_iota(jnp.int32, (rows, slots), 0)
    s_i = lax.broadcasted_iota(jnp.int32, (rows, slots), 1)
    squeeze = jnp.where(s_i == (r_i // cap) * PAD + r_i % cap, 1.0, 0.0).astype(BF16)
    for k in range(NCHUNK):
        cols = pl.ds(k * cw, cw)
        wait_bytes(chunk_bytes(dispatched, k), disp_recv.at[k])
        came = dispatched[:, :, cols].reshape(slots, cw)
        blocks[pl.ds(c, 1), pl.ds(z, 1), :, cols] = (
            jnp.dot(squeeze, came, preferred_element_type=F32)
            .astype(BF16)
            .reshape(1, 1, rows, cw)
        )
        gather_copy(0, k).start()
    pair_copy(0).start()
    for load in loads[8:]:
        load.wait()
    own_q = rotated(qt_ref[...].astype(F32), column(q_gain), cosines, sines).astype(BF16)
    for g in range(seg // q_width):
        qt[g, 0:hd, :] = own_q[:, g * q_width : (g + 1) * q_width]
        qt[g, hd : 2 * hd, :] = jnp.zeros((hd, q_width), BF16)
    peak[...] = jnp.full(peak.shape, -jnp.inf, F32)
    acc[...] = jnp.zeros(acc.shape, F32)

    def half_bytes(n):
        return kv.at[pl.ds(0, n), pl.ds(0, seg // 2), :]

    def kv_forward(g):
        wait_bytes(half_bytes(KV_GROUP), kv_recv.at[g])
        for i in range(KV_GROUP):
            kv_pair_copy(g * KV_GROUP + 1 + i).start()

    def gather_step(s, carry):
        def forward(k):
            gather_copy(s, k).wait_recv()
            gather_copy(s + 1, k).start()

        forward(0)

        @pl.when(s == 0)
        def _():
            each(lambda d: kv_copy(d).start())

        forward(1)
        feed_own(s)
        forward(2)

        @pl.when(s >= KV_FROM)
        def _():
            kv_forward(s - KV_FROM)

        feed_partner(s)
        forward(3)
        pair_copy(s + 1).start()
        return carry

    lax.fori_loop(0, last - 1, gather_step, 0)

    def first_hop(k):
        b = at_z(-way)
        cols = pl.ds(k * cw, cw)
        value = parts[pl.ds(c, 1), pl.ds(b, 1), :, cols].astype(F32).reshape(rows, cw)
        value += partner_parts[pl.ds(b, 1), :, cols].astype(F32).reshape(rows, cw)
        parts[pl.ds(c, 1), pl.ds(b, 1), :, cols] = value.astype(BF16).reshape(1, 1, rows, cw)
        reduce_copy(0, k).start()

    part_copy(1).wait_recv()
    for k in range(NCHUNK):
        first_hop(k)
    feed_own(last - 1)
    feed_partner(last - 1)
    for k in range(NCHUNK):
        gather_copy(last - 1, k).wait_recv()
    pair_copy(last).start()
    for g in range(last - 1 - KV_FROM, (n_ep - 1) // KV_GROUP):
        kv_forward(g)
    feed_own(last)
    feed_partner(last)

    def turn(j, carry):
        cols = pl.ds(pl.multiple_of(j * seg, seg), seg)
        vt[0:hd, cols] = kv[pl.ds(j, 1)].reshape(seg, 2 * hd).T[hd : 2 * hd]
        vt[hd : hd + 16, cols] = jnp.ones((16, seg), BF16)
        return carry

    def reduce_step(s, carry):
        b = at_z(-way * (s + 1))
        part_copy(s + 1).wait_recv()
        for k in range(NCHUNK):
            cols = pl.ds(k * cw, cw)
            value = parts[pl.ds(c, 1), pl.ds(b, 1), :, cols].astype(F32).reshape(rows, cw)
            value += partner_parts[pl.ds(b, 1), :, cols].astype(F32).reshape(rows, cw)
            reduce_copy(s - 1, k).wait_recv()
            value += ring_in[pl.ds(s - 1, 1), :, cols].astype(F32).reshape(rows, cw)
            parts[pl.ds(c, 1), pl.ds(b, 1), :, cols] = value.astype(BF16).reshape(1, 1, rows, cw)
            reduce_copy(s, k).start()

            @pl.when(s > 1)
            def _():
                for i in range(PIECES[k], PIECES[k + 1]):
                    piece((s - 2) * PIECES[-1] + i)

        @pl.when(s == 1)
        def _():
            wait_bytes(half_bytes(n_ep - 1), kvp_recv.at[0])
            lax.fori_loop(0, n_ep, turn, 0)
            top[...] = score(0, s0)

        return carry

    lax.fori_loop(1, last, reduce_step, 0)

    r_j = lax.broadcasted_iota(jnp.int32, (slots, rows), 1)
    s_j = lax.broadcasted_iota(jnp.int32, (slots, rows), 0)
    spread = jnp.where(s_j == (r_j // cap) * PAD + r_j % cap, 1.0, 0.0).astype(BF16)
    wait_bytes(outgoing.at[pl.ds(0, n_ep - 1)], disp_send.at[0])
    part_copy(0).wait_recv()
    done = (last - 2) * PIECES[-1]
    extra = -(-(tiles // 2 - done) // NCHUNK)
    for k in range(NCHUNK):
        cols = pl.ds(k * cw, cw)
        value = parts[pl.ds(c, 1), pl.ds(z, 1), :, cols].astype(F32).reshape(rows, cw)
        value += partner_parts[pl.ds(z, 1), :, cols].astype(F32).reshape(rows, cw)
        reduce_copy(last - 1, k).wait_recv()
        value += ring_in[last - 1, :, cols].astype(F32)
        outgoing[:, :, cols] = (
            jnp.dot(spread, value.astype(BF16), preferred_element_type=F32)
            .astype(BF16)
            .reshape(n_ep, PAD, cw)
        )
        returned[pl.ds(e, 1), :, cols] = outgoing[pl.ds(e, 1), :, cols]
        each(lambda d: give_back(d, k).start())
        for i in range(done + k * extra, min(done + (k + 1) * extra, tiles // 2)):
            piece(i)

    for g in range(seg // q_width):
        att_ref[:, g * q_width : (g + 1) * q_width] = (
            acc[g, 0:hd, :] / acc[g, hd : hd + 1, :]
        ).astype(BF16)

    wait_bytes(half_bytes(n_ep - 1), kv_send.at[0])
    wait_bytes(half_bytes(n_ep - 1), kvp_send.at[0])
    wait_bytes(blocks.at[0], pair_send.at[0])
    wait_bytes(blocks.at[0], part_send.at[0])
    wait_bytes(blocks.at[0, pl.ds(0, last)], gath_send.at[0])
    wait_bytes(blocks.at[0, pl.ds(0, last)], red_send.at[0])

    lane_s = lax.broadcasted_iota(jnp.int32, (tokens, slots), 1).astype(F32)
    ones = [jnp.where(lane_s == col, 1.0, 0.0).astype(BF16) for col in slot_cols]
    shares = [own_t[0:tokens, top_count + k : top_count + k + 1] for k in range(top_count)]
    mean = jnp.zeros((tokens, 1), F32)
    for k in range(NCHUNK):
        cols = pl.ds(k * cw, cw)
        wait_bytes(chunk_bytes(returned, k), ret_recv.at[k])
        back = returned[:, :, cols].reshape(slots, cw)
        both = None
        for one, share in zip(ones, shares):
            term = share * jnp.dot(one, back, preferred_element_type=F32)
            both = term if both is None else both + term
        part = residual_scale * x_ref[:, cols].astype(F32) + both
        mixed[:, cols] = part
        mean += jnp.sum(part, axis=-1, keepdims=True)
    centered = mixed[...] - mean / width
    variance = jnp.mean(centered * centered, axis=-1, keepdims=True)
    out_ref[...] = (centered * lax.rsqrt(variance + norm_epsilon) * gain_ref[...]).astype(BF16)
    wait_bytes(outgoing.at[pl.ds(0, n_ep - 1)], ret_send.at[0])


def layer(ids, route, x, gain, qt, q_gain, k_gain, keys, values, gate_t, up_t, down,
          n_ep, n_z, cap, group):
    tokens, width = x.shape
    hidden = down.shape[0]
    head_size, seg = qt.shape
    rows = n_ep * cap
    vmem = pl.BlockSpec(memory_space=pltpu.VMEM)
    hbm = pl.BlockSpec(memory_space=pltpu.HBM)
    dma = pltpu.SemaphoreType.DMA
    hops = (n_z - 1) * NCHUNK
    groups = seg // Q_WIDTH
    return pl.pallas_call(
        functools.partial(layer_kernel, n_ep, n_z, group),
        out_shape=(
            pltpu.VMEM((head_size, seg), BF16),
            pltpu.VMEM((tokens, width), BF16),
        ),
        in_specs=[hbm] * 12,
        out_specs=(vmem, vmem),
        scratch_shapes=[
            pltpu.VMEM(ids.shape, ids.dtype),
            pltpu.VMEM(route.shape, F32),
            pltpu.VMEM((tokens, width), BF16),
            pltpu.VMEM((1, width), F32),
            pltpu.VMEM((head_size, seg), BF16),
            pltpu.VMEM((1, head_size), F32),
            pltpu.VMEM((1, head_size), F32),
            pltpu.VMEM((hidden, width), BF16),
            pltpu.VMEM((hidden, width), BF16),
            pltpu.VMEM((width, hidden), BF16),
            pltpu.VMEM((width, hidden), BF16),
            pltpu.VMEM((hidden, width), BF16),
            pltpu.VMEM((seg, 2 * head_size), BF16),
            pltpu.VMEM((seg, 2 * head_size), BF16),
            pltpu.VMEM((n_ep, seg, 2 * head_size), BF16),
            pltpu.VMEM((head_size + 16, n_ep * seg), BF16),
            pltpu.VMEM((groups, 2 * head_size, Q_WIDTH), BF16),
            pltpu.VMEM((K_BLOCK, Q_WIDTH), F32),
            pltpu.VMEM((K_BLOCK, Q_WIDTH), F32),
            pltpu.VMEM((1, Q_WIDTH), F32),
            pltpu.VMEM((groups, 1, Q_WIDTH), F32),
            pltpu.VMEM((groups, head_size + 16, Q_WIDTH), F32),
            pltpu.VMEM((n_ep, PAD, width), BF16),
            pltpu.VMEM((n_ep, PAD, width), BF16),
            pltpu.VMEM((2, n_z, rows, width), BF16),
            pltpu.VMEM((2, n_z, rows, width), BF16),
            pltpu.VMEM((n_z, rows, width), BF16),
            pltpu.VMEM((n_z - 1, rows, width), BF16),
            pltpu.VMEM((n_ep, PAD, width), BF16),
            pltpu.VMEM((tokens, width), F32),
            pltpu.VMEM((8, ids.shape[1]), F32),
            dma((12,)),
            dma((1,)),
            dma((NCHUNK,)),
            dma((1,)),
            dma((hops,)),
            dma((1,)),
            dma((n_z,)),
            dma((1,)),
            dma((n_z,)),
            dma((1,)),
            dma((hops,)),
            dma((1,)),
            dma((NCHUNK,)),
            dma((1,)),
            dma(((n_ep - 1) // KV_GROUP,)),
            dma((1,)),
            dma((1,)),
        ],
        compiler_params=pltpu.CompilerParams(
            collective_id=0, has_side_effects=True, vmem_limit_bytes=VMEM_LIMIT
        ),
    )(ids, route, x, gain, qt, q_gain, k_gain, keys, values, gate_t, up_t, down)


def shards(
    queries,
    keys,
    values,
    query_gain,
    key_gain,
    moe_input,
    expert_ids,
    route_weight,
    gate_weight,
    up_weight,
    down_weight,
    output_gain,
):
    tok_rows = moe_input.shape[0]
    top_count = expert_ids.shape[1]
    n_ep = lax.axis_size("ep")
    n_tp = lax.axis_size("tp")
    cap = max(2, tok_rows * top_count * 5 // (4 * n_ep))
    attended, moe_output = layer(
        expert_ids.T,
        route_weight.T,
        moe_input,
        output_gain[None, :],
        queries.T,
        query_gain[None, :],
        key_gain[None, :],
        keys,
        values,
        gate_weight[0].T,
        up_weight[0].T,
        down_weight[0],
        n_ep,
        n_tp // 2,
        cap,
        QH // KV,
    )
    return (attended.T, moe_output)


def solution(mesh):
    return jax.shard_map(
        shards,
        mesh=mesh,
        in_specs=(
            P("ep", "tp"),
            P("ep", None),
            P("ep", None),
            P(),
            P(),
            P(("ep", "tp"), None),
            P("ep", None),
            P("ep", None),
            P("ep", None, "tp"),
            P("ep", None, "tp"),
            P("ep", "tp", None),
            P(),
        ),
        out_specs=(P("ep", "tp"), P(("ep", "tp"), None)),
        check_vma=False,
    )
```
